32 devices in a mesh: fs: 8 (over z, x), tp: 4 (over y, core).
Axes of the slice: x: 2, y: 2, z: 4, core: 2. Of those that a mesh axis runs over, the one named last changes fastest.
Arguments:
- normed_input: bfloat16 [16384, 2048], P('fs'), may hold values from -6 to 6
- gate_cotangent: bfloat16 [16384, 2048], P('fs', 'tp'), may hold values from -0.125 to 0.125
- first_value_cot: bfloat16 [16384, 1024], P('fs', 'tp'), may hold values from -0.125 to 0.125
- second_value_cot: bfloat16 [16384, 1024], P('fs', 'tp'), may hold values from -0.125 to 0.125
- head_lambda: float32 [8], P('tp'), may hold values from 0.3 to 0.8
- projection: bfloat16 [2048, 256], replicated, may hold values from -1 to 1, as said below
- gate_weight: float32 [2048, 2048], P('fs', 'tp'), may hold values from -0.125 to 0.125
- gate_first: float32 [256, 2048], P('fs', 'tp'), may hold values from -1.5 to 1.5
- gate_second: float32 [256, 2048], P('fs', 'tp'), may hold values from 0.01 to 1
- value_weight: float32 [2048, 1024], P('fs', 'tp'), may hold values from -0.125 to 0.125
- value_first: float32 [256, 1024], P('fs', 'tp'), may hold values from -1.5 to 1.5
- value_second: float32 [256, 1024], P('fs', 'tp'), may hold values from 0.01 to 1
Outputs:
- new_gate_weight: float32 [2048, 2048], P('fs', 'tp')
- gate_step: float32 [2048, 2048], P('fs', 'tp')
- gate_copy: bfloat16 [2048, 2048], P(None, 'tp')
- new_gate_first: float32 [256, 2048], P('fs', 'tp')
- new_gate_second: float32 [256, 2048], P('fs', 'tp')
- new_value_weight: float32 [2048, 1024], P('fs', 'tp')
- value_step: float32 [2048, 1024], P('fs', 'tp')
- value_copy: bfloat16 [2048, 1024], P(None, 'tp')
- new_value_first: float32 [256, 1024], P('fs', 'tp')
- new_value_second: float32 [256, 1024], P('fs', 'tp')
The draws below stay inside these ranges and needn't reach their ends.
Inputs may be any that keep to these rules, and one draw needn't show every extreme that they name: `projection`: a low-rank factor whose rows differ in scale.
All inputs are finite; a program needn't handle non-finite values.
Results may differ from the reference program's by a relative error of at most 0.0054.
Values may be sent and summed in bfloat16 or wider, within the bound.
A program may use at most 64 MiB of HBM per device.

```python
import math
import jax
import jax.numpy as jnp
from jax import lax

D = 2048
HEADS = 8
VDIM = 128
RANK = 256
TOKENS = 16384


def draw_projection(key, part):
    noise_key = jax.random.fold_in(key, 11)
    rough_key = jax.random.fold_in(key, 12)
    phase_key = jax.random.fold_in(key, 13)
    row_place = jnp.arange(D, dtype=jnp.float32)[:, None] / D
    phase = jax.random.uniform(phase_key, (), jnp.float32, 0.0, 6.2832)
    slow = jnp.exp(1.2 * jnp.sin(12.566 * row_place + phase))
    rough = jnp.exp(jax.random.uniform(rough_key, (D, 1), jnp.float32, -0.5, 0.5))
    base = jax.random.normal(noise_key, (D, RANK), jnp.float32)
    value = base * slow * rough * D ** (-0.5)
    return jnp.clip(value, -1.0, 1.0).astype(jnp.bfloat16)


def raised(entries, key, source, target, shards_of, factor):
    owner, partner = [(jnp.arange(entries.shape[axis_at]) // (entries.shape[axis_at] // shards_of)).reshape([-1 if axis == axis_at else 1 for axis in range(entries.ndim)]) for axis_at in (source, target)]
    chosen = jax.random.permutation(key, shards_of)[partner]
    strong = (owner == chosen) | (owner == (partner + shards_of // 2) % shards_of)
    return jnp.where(strong, factor * entries, entries)


def steps_of(key, dims, split, smallest, largest):
    loudness = 1.0
    for axis_at, blocks in split:
        heights = jax.random.uniform(jax.random.fold_in(jax.random.fold_in(key, 6), axis_at), (blocks,), jnp.float32, smallest / len(split), largest / len(split))
        loudness = loudness * jnp.repeat(jnp.exp(heights), dims[axis_at] // blocks).reshape((-1,) + (1,) * (len(dims) - 1 - axis_at))
    return loudness


def noise(own_key, dims, spread, bound, cuts=(), held_as=jnp.bfloat16):
    array = spread * jax.random.normal(own_key, dims, jnp.float32)
    if cuts:
        array = array * steps_of(own_key, dims, cuts, -0.22, 0.18)
    return jnp.clip(array, -bound, bound).astype(held_as)


def gaussian_with(key, extent, deviation, limit, shards, heavy, kind=jnp.bfloat16):
    array = deviation * jax.random.normal(key, extent, jnp.float32)
    if shards:
        array = array * steps_of(key, extent, shards, -0.22, 0.18)
    return jnp.clip(raised(array, jax.random.fold_in(key, 3), *heavy), -limit, limit).astype(kind)


def setup_inputs(seed: int = 0) -> dict:
    splits = jax.random.split(jax.random.key(seed), 13)
    return {
        "normed_input": gaussian_with(splits[0], (TOKENS, D), 1.0, 6.0, ((0, 8),), (0, 1, 8, 2.0)),
        "gate_cotangent": noise(splits[1], (TOKENS, D), (TOKENS ** -0.5), 0.125, ((0, 8), (1, 4))),
        "first_value_cot": noise(splits[2], (TOKENS, HEADS * VDIM), (TOKENS ** -0.5), 0.125, ((0, 8), (1, 4))),
        "second_value_cot": noise(splits[3], (TOKENS, HEADS * VDIM), (TOKENS ** -0.5), 0.125, ((0, 8), (1, 4))),
        "head_lambda": jnp.clip(0.3 + 0.5 * jax.random.uniform(splits[4], (HEADS,), jnp.float32) ** steps_of(splits[4], (HEADS,), ((0, 4),), -0.2, 0.2), 0.3, 0.8),
        "projection": draw_projection(jax.random.fold_in(splits[12], 71), 0),
        "gate_weight": noise(splits[6], (D, D), D ** -0.5, 0.125, ((0, 8), (1, 4)), jnp.float32),
        "gate_first": noise(splits[7], (RANK, D), 0.1, 1.5, ((0, 8), (1, 4)), jnp.float32),
        "gate_second": jnp.clip(jnp.exp(math.log(1.0) - 4.6051702 * jax.random.uniform(splits[8], (RANK, D), jnp.float32) ** steps_of(splits[8], (RANK, D), ((0, 8), (1, 4)), -0.2, 0.2)), 0.01, 1.0),
        "value_weight": noise(splits[9], (D, HEADS * VDIM), D ** -0.5, 0.125, ((0, 8), (1, 4)), jnp.float32),
        "value_first": noise(splits[10], (RANK, HEADS * VDIM), 0.1, 1.5, ((0, 8), (1, 4)), jnp.float32),
        "value_second": jnp.clip(jnp.exp(math.log(1.0) - 4.6051702 * jax.random.uniform(splits[11], (RANK, HEADS * VDIM), jnp.float32) ** steps_of(splits[11], (RANK, HEADS * VDIM), ((0, 8), (1, 4)), -0.2, 0.2)), 0.01, 1.0),
    }


moment_decay = 0.9
square_decay = 0.95
adam_floor = 1e-08
learn_rate = 0.02
rms_floor = 0.1

def across_tokens(left, right):
    return lax.dot_general(left, right, (((0,), (0,)), ((), ())), preferred_element_type=jnp.float32)

def optimizer_step(weight, first, second, gradient, projection):
    factor = projection.astype(jnp.float32)
    low = lax.dot_general(factor, gradient, (((0,), (0,)), ((), ())), precision=lax.Precision.HIGHEST)
    new_first = moment_decay * first + (1.0 - moment_decay) * low
    new_second = square_decay * second + (1.0 - square_decay) * low * low
    direction = new_first / (jnp.sqrt(new_second) + adam_floor)
    update = jnp.dot(factor, direction, precision=lax.Precision.HIGHEST)
    step = update / (jnp.sqrt(jnp.mean(update * update)) + rms_floor)
    new_weight = weight - learn_rate * step
    return (new_weight, step, new_weight.astype(jnp.bfloat16), new_first, new_second)

def reference(normed_input, gate_cotangent, first_value_cot, second_value_cot, head_lambda, projection, gate_weight, gate_first, gate_second, value_weight, value_first, value_second):
    column_lambda = jnp.repeat(head_lambda, VDIM)
    value_cot = (first_value_cot.astype(jnp.float32) - column_lambda[None, :] * second_value_cot.astype(jnp.float32)).astype(jnp.bfloat16)
    gate_grad = across_tokens(normed_input, gate_cotangent)
    value_grad = across_tokens(normed_input, value_cot)
    gate_parts = optimizer_step(gate_weight, gate_first, gate_second, gate_grad, projection)
    value_parts = optimizer_step(value_weight, value_first, value_second, value_grad, projection)
    return (gate_parts[0], gate_parts[1], gate_parts[2], gate_parts[3], gate_parts[4], value_parts[0], value_parts[1], value_parts[2], value_parts[3], value_parts[4])
```

```python
import functools

import jax
import jax.numpy as jnp
from jax import lax
from jax.experimental import pallas as pl
from jax.experimental.pallas import tpu as pltpu
from jax.sharding import PartitionSpec as P

VDIM = 128
PIECES = 8
PIECE_ROWS = 16
CROSS = 1
CHUNKS = 4
STEP_TOKENS = 256
HOLD_X = 4
HOLD_ONE = 6
HOLD_TWO = 4
HOLD_THREE = 4

moment_decay = 0.9
square_decay = 0.95
adam_floor = 1e-08
learn_rate = 0.02
rms_floor = 0.1

MESH = pl.DeviceIdType.MESH
f32, bf16 = jnp.float32, jnp.bfloat16


def factor_fs(count):
    inner = 1
    while (2 * inner) ** 2 <= count and count % (2 * inner) == 0:
        inner *= 2
    return count // inner, inner


def kernel(
    nz,
    nx,
    nt,
    x_hbm,
    gcot_hbm,
    fcot_hbm,
    scot_hbm,
    lam_hbm,
    proj_hbm,
    gw_hbm,
    gm_hbm,
    gs_hbm,
    vw_hbm,
    vm_hbm,
    vs_hbm,
    new_gw,
    gsteps,
    gcopy,
    new_gm,
    new_gs,
    new_vw,
    vsteps,
    vcopy,
    new_vm,
    new_vs,
    lam_ref,
    xv,
    gcv,
    fcv,
    scv,
    pv,
    gw,
    vw,
    gm,
    gs,
    vm,
    vs,
    wall,
    acc,
    updates,
    rsrc,
    rsx,
    zsrc,
    rsz,
    dall,
    dcat,
    sums,
    in_sem,
    x_sem,
    wz_send,
    wz_recv,
    wx_send,
    wx_recv,
    rx_send,
    rx_recv,
    rz_send,
    rz_recv,
    dz_send,
    dz_recv,
    dx_send,
    dx_recv,
    t_send,
    t_recv,
):
    nfs = nz * nx
    f = lax.axis_index("fs")
    t = lax.axis_index("tp")
    z = lax.div(f, nx)
    x = lax.rem(f, nx)
    rows, cg = gw.shape
    cv = vw.shape[1]
    cols = cg + cv
    rank = acc.shape[0]
    share = rank // nfs
    pieces, part = wall.shape[1:3]
    tokens = x_hbm.shape[0] // CHUNKS
    cross = range(pieces * CROSS // 8)
    direct = range(len(cross), pieces)
    items = [(0, p) for p in range(pieces)] + [(k, p) for p in cross for k in range(1, nx)]

    def zpeer(k):
        return lax.rem(z + k, nz)

    def xpeer(k):
        return lax.rem(x + k, nx)

    barrier = pltpu.get_barrier_semaphore()
    for k in range(1, nz):
        pl.semaphore_signal(barrier, inc=1, device_id=(zpeer(k) * nx + x, t), device_id_type=MESH)
    for k in range(1, nx):
        pl.semaphore_signal(barrier, inc=1, device_id=(z * nx + xpeer(k), t), device_id_type=MESH)
    for k in range(1, nt):
        pl.semaphore_signal(barrier, inc=1, device_id=(f, lax.rem(t + k, nt)), device_id_type=MESH)

    small = [
        pltpu.make_async_copy(src, dst, in_sem.at[i])
        for i, (src, dst) in enumerate(
            [
                (gw_hbm, gw),
                (vw_hbm, vw),
                (proj_hbm, pv),
                (gm_hbm, gm),
                (gs_hbm, gs),
                (vm_hbm, vm),
                (vs_hbm, vs),
                (lam_hbm, lam_ref),
            ]
        )
        if src is not lam_hbm or cv > VDIM
    ]
    if cv == VDIM:
        lam_ref = lam_hbm

    def chunk_copies(c):
        at = pl.ds(c * tokens, tokens)
        return [
            pltpu.make_async_copy(src.at[at], dst.at[at], x_sem.at[i, c])
            for i, (src, dst) in enumerate(
                [(x_hbm, xv), (gcot_hbm, gcv), (fcot_hbm, fcv), (scot_hbm, scv)]
            )
        ]

    for copy in small[:3] + small[7:]:
        copy.start()
    for c in range(CHUNKS):
        for copy in chunk_copies(c):
            copy.start()
    for i in range(3, 7):
        small[i].start()

    small[0].wait()
    small[1].wait()
    for p in range(pieces):
        at = pl.ds(p * part, part)
        wall[f, p, :, :cg] = gw[at, :].astype(bf16)
        wall[f, p, :, cg:] = vw[at, :].astype(bf16)

    def valid(row):
        return jnp.logical_and(row >= 0, row < nz)

    def wz(way, src_z, i, peer):
        k, p = items[i]
        owner = src_z * nx + xpeer(k)
        return pltpu.make_async_remote_copy(
            src_ref=wall.at[owner, p],
            dst_ref=wall.at[owner, p],
            send_sem=wz_send.at[(way + 1) // 2, src_z, i],
            recv_sem=wz_recv.at[src_z, i],
            device_id=(peer * nx + x, t),
            device_id_type=MESH,
        )

    def wx(k, p, src_z, src_x):
        owner = src_z * nx + src_x
        return pltpu.make_async_remote_copy(
            src_ref=wall.at[owner, p],
            dst_ref=wall.at[owner, p],
            send_sem=wx_send.at[k, src_z, p],
            recv_sem=wx_recv.at[src_x, src_z, p],
            device_id=(z * nx + xpeer(k), t),
            device_id_type=MESH,
        )

    def along(way, src_z, i):
        @pl.when(valid(z + way))
        def _():
            wz(way, src_z, i, z + way).start()

    def over(src_z, p):
        for k in range(1, nx):
            wx(k, p, src_z, x).start()

    def relay(step, i):
        k, p = items[i]
        for way in (1, -1):
            src_z = z - way * step

            @pl.when(valid(src_z))
            def _():
                wz(way, src_z, i, z - way).wait_recv()
                along(way, src_z, i)
                if k == 0 and p in direct:
                    over(src_z, p)

    def cross_over():
        for i in range(pieces, len(items)):
            k, p = items[i]
            wx(k, p, z, xpeer(k)).wait_recv()
            for way in (1, -1):
                along(way, z, i)

    pl.semaphore_wait(barrier, (nz - 1) + (nx - 1) + (nt - 1))
    for p in cross:
        over(z, p)
    for p in range(pieces):
        for way in (1, -1):
            along(way, z, p)
        if p in direct and p < HOLD_X:
            over(z, p)

    for copy in small[2:3] + small[7:]:
        copy.wait()
    acc[...] = jnp.zeros_like(acc)
    head = lax.broadcasted_iota(jnp.int32, (1, cv), 1) // VDIM
    lam = jnp.zeros((1, cv), f32)
    for h in range(cv // VDIM):
        lam = jnp.where(head == h, lam_ref[h], lam)
    for c in range(CHUNKS):
        for copy in chunk_copies(c):
            copy.wait()

        def multiply(i, carry):
            at = pl.ds(pl.multiple_of(c * tokens + i * STEP_TOKENS, STEP_TOKENS), STEP_TOKENS)
            upper = jnp.dot(xv[at, :], pv[...], preferred_element_type=f32).astype(bf16)
            value = (fcv[at, :].astype(f32) - lam * scv[at, :].astype(f32)).astype(bf16)
            across = (((0,), (0,)), ((), ()))
            acc[:, :cg] += lax.dot_general(upper, gcv[at, :], across, preferred_element_type=f32)
            acc[:, cg:] += lax.dot_general(upper, value, across, preferred_element_type=f32)
            return carry

        lax.fori_loop(0, tokens // STEP_TOKENS, multiply, 0)

    for zi in range(nz):
        for xi in range(nx):
            at = pl.ds((zi * nx + xi) * share, share)
            rsrc[xi, zi] = acc[at, :].astype(bf16)

    def rx(k, src_x, dst_x):
        return pltpu.make_async_remote_copy(
            src_ref=rsrc.at[dst_x],
            dst_ref=rsx.at[src_x],
            send_sem=rx_send.at[k],
            recv_sem=rx_recv.at[src_x],
            device_id=(z * nx + xpeer(k), t),
            device_id_type=MESH,
        )

    for k in range(1, nx):
        rx(k, x, xpeer(k)).start()
    cross_over()
    for p in direct:
        if p >= HOLD_X:
            over(z, p)

    def relays(step, lo, hi):
        if step < nz:
            for i in range(min(lo, len(items)), min(hi, len(items))):
                relay(step, i)

    relays(1, 0, HOLD_ONE)
    for k in range(1, nx):
        rx(k, xpeer(k), x).wait_recv()
    for zi in range(nz):
        at = pl.ds(pl.multiple_of((zi * nx + x) * share, share), share)
        total = acc[at, :]
        for k in range(1, nx):
            total = total + rsx[xpeer(k), zi].astype(f32)
        zsrc[zi] = total.astype(bf16)

    def rz(k, src_z, dst_z):
        return pltpu.make_async_remote_copy(
            src_ref=zsrc.at[dst_z],
            dst_ref=rsz.at[src_z],
            send_sem=rz_send.at[k],
            recv_sem=rz_recv.at[src_z],
            device_id=(zpeer(k) * nx + x, t),
            device_id_type=MESH,
        )

    for k in range(1, nz):
        rz(k, z, zpeer(k)).start()
    relays(1, HOLD_ONE, len(items))
    relays(2, 0, HOLD_TWO)
    for i in range(3, 7):
        small[i].wait()
    low = zsrc[z].astype(f32)
    for k in range(1, nz):
        rz(k, zpeer(k), z).wait_recv()
        low = low + rsz[zpeer(k)].astype(f32)

    for first, second, new_m, new_s, at in (
        (gm, gs, new_gm, new_gs, slice(0, cg)),
        (vm, vs, new_vm, new_vs, slice(cg, cols)),
    ):
        mine = low[:, at]
        new_first = moment_decay * first[...] + (1.0 - moment_decay) * mine
        new_second = square_decay * second[...] + (1.0 - square_decay) * mine * mine
        new_m[...] = new_first
        new_s[...] = new_second
        dall[f, :, at] = (new_first / (jnp.sqrt(new_second) + adam_floor)).astype(bf16)

    def dz(k, src_z):
        owner = src_z * nx + x
        return pltpu.make_async_remote_copy(
            src_ref=dall.at[owner],
            dst_ref=dall.at[owner],
            send_sem=dz_send.at[k],
            recv_sem=dz_recv.at[src_z],
            device_id=(zpeer(k) * nx + x, t),
            device_id_type=MESH,
        )

    def dx(k, src_z, src_x):
        owner = src_z * nx + src_x
        return pltpu.make_async_remote_copy(
            src_ref=dall.at[owner],
            dst_ref=dall.at[owner],
            send_sem=dx_send.at[k, src_z],
            recv_sem=dx_recv.at[src_x, src_z],
            device_id=(z * nx + xpeer(k), t),
            device_id_type=MESH,
        )

    for k in range(1, nz):
        dz(k, z).start()
    for m in range(1, nx):
        dx(m, z, x).start()
    relays(2, HOLD_TWO, len(items))
    for k in range(1, nz):
        dz(k, zpeer(k)).wait_recv()
        for m in range(1, nx):
            dx(m, zpeer(k), x).start()
    relays(3, 0, HOLD_THREE)
    for m in range(1, nx):
        for zi in range(nz):
            dx(m, zi, xpeer(m)).wait_recv()

    for j in range(nfs):
        dcat[pl.ds(j * share, share), :] = dall[j].astype(f32)
    direction = dcat[...].astype(bf16)

    def expand(j, squares):
        at = pl.ds(pl.multiple_of(j * rows, rows), rows)
        block = jnp.dot(pv[at, :], direction, preferred_element_type=f32)
        updates[at, :] = block
        return squares + jnp.sum((block * block).reshape(rows // 8, 8, cols), axis=0)

    squares = lax.fori_loop(0, nfs, expand, jnp.zeros((8, cols), f32))
    squares = jnp.sum(squares, axis=0, keepdims=True)
    gate_sum = jnp.sum(squares[:, :cg], axis=1, keepdims=True)
    value_sum = jnp.sum(squares[:, cg:], axis=1, keepdims=True)
    sums[t, 0] = jnp.broadcast_to(gate_sum, (8, 128))
    sums[t, 1] = jnp.broadcast_to(value_sum, (8, 128))

    def tp(k, src_t):
        return pltpu.make_async_remote_copy(
            src_ref=sums.at[src_t],
            dst_ref=sums.at[src_t],
            send_sem=t_send.at[k],
            recv_sem=t_recv.at[src_t],
            device_id=(f, lax.rem(t + k, nt)),
            device_id_type=MESH,
        )

    for k in range(1, nt):
        tp(k, t).start()
    relays(3, HOLD_THREE, len(items))
    for step in range(4, nz):
        relays(step, 0, len(items))
    for k in range(1, nt):
        tp(k, lax.rem(t + k, nt)).wait_recv()
    whole = sums[0]
    for k in range(1, nt):
        whole = whole + sums[k]
    entries = nfs * rows * nt
    gscale = (1.0 / (jnp.sqrt(whole[0] / (entries * cg)) + rms_floor))[0:1, 0:1]
    vscale = (1.0 / (jnp.sqrt(whole[1] / (entries * cv)) + rms_floor))[0:1, 0:1]

    at = pl.ds(pl.multiple_of(f * rows, rows), rows)
    gstep = updates[at, :cg] * gscale
    vstep = updates[at, cg:] * vscale
    gsteps[...] = gstep
    vsteps[...] = vstep
    new_gw[...] = gw[...] - learn_rate * gstep
    new_vw[...] = vw[...] - learn_rate * vstep

    def finish(j, p):
        at = pl.ds(pl.multiple_of(j * rows + p * part, part), part)
        held = wall[j, p].astype(f32)
        update = updates[at, :]
        gcopy[at, :] = (held[:, :cg] - learn_rate * (update[:, :cg] * gscale)).astype(bf16)
        vcopy[at, :] = (held[:, cg:] - learn_rate * (update[:, cg:] * vscale)).astype(bf16)

    def finish_block(j, lo, hi):
        def body(p, carry):
            finish(j, p)
            return carry

        lax.fori_loop(lo, hi, body, 0)

    for zi in range(nz):
        finish_block(zi * nx + x, 0, pieces)
        if len(cross):
            for k in range(1, nx):
                finish_block(zi * nx + xpeer(k), 0, len(cross))
    for step in range(nz):
        for p in direct:
            for way in (1, -1) if step else (1,):
                src_z = z - way * step

                @pl.when(valid(src_z))
                def _():
                    for k in range(1, nx):
                        wx(k, p, src_z, xpeer(k)).wait_recv()
                        finish(src_z * nx + xpeer(k), p)

    for way in (1, -1):
        for step in range(nz):
            src_z = z - way * step

            @pl.when(jnp.logical_and(valid(src_z), valid(z + way)))
            def _():
                for i in range(len(items)):
                    wz(way, src_z, i, z + way).wait_send()

    for m in range(1, nx):
        for p in cross:
            wx(m, p, z, x).wait_send()
        for zi in range(nz):
            for p in direct:
                wx(m, p, zi, x).wait_send()
            dx(m, zi, x).wait_send()
        rx(m, x, xpeer(m)).wait_send()
    for k in range(1, nz):
        rz(k, z, zpeer(k)).wait_send()
        dz(k, z).wait_send()
    for k in range(1, nt):
        tp(k, t).wait_send()


def put_kernel(*refs):
    count = (len(refs) - 1) // 2
    sem = refs[-1]
    copies = [pltpu.make_async_copy(refs[i], refs[count + i], sem.at[i]) for i in range(count)]
    for copy in copies:
        copy.start()
    for copy in copies:
        copy.wait()


def per_device(nz, nx, nt, xin, gcot, fcot, scot, lam, proj, gw, gm, gs, vw, vm, vs):
    nfs = nz * nx
    rows, cg = gw.shape
    cv = vw.shape[1]
    cols = cg + cv
    depth, rank = proj.shape
    share = rank // nfs
    pieces = min(PIECES, rows // PIECE_ROWS)
    part = rows // pieces
    items = pieces + (nx - 1) * (pieces * CROSS // 8)
    dma = pltpu.SemaphoreType.DMA
    shape = jax.ShapeDtypeStruct
    vmem = lambda a: pltpu.VMEM(a.shape, a.dtype)
    results = [
        shape((rows, cg), f32),
        shape((rows, cg), f32),
        shape((depth, cg), bf16),
        shape(gm.shape, f32),
        shape(gs.shape, f32),
        shape((rows, cv), f32),
        shape((rows, cv), f32),
        shape((depth, cv), bf16),
        shape(vm.shape, f32),
        shape(vs.shape, f32),
    ]
    arrays = [xin, gcot, fcot, scot, lam, proj, gw, gm, gs, vw, vm, vs]
    alone = cv == VDIM
    arrays = [
        a if alone and a is lam else pltpu.with_memory_space_constraint(a, pltpu.HBM)
        for a in arrays
    ]
    anywhere = pl.BlockSpec(memory_space=pl.ANY)
    inside = pl.BlockSpec(memory_space=pltpu.VMEM)
    held = pl.pallas_call(
        functools.partial(kernel, nz, nx, nt),
        out_shape=[vmem(a) for a in results],
        in_specs=[
            pl.BlockSpec(memory_space=pltpu.SMEM) if alone and a is lam else anywhere
            for a in (xin, gcot, fcot, scot, lam, proj, gw, gm, gs, vw, vm, vs)
        ],
        out_specs=[inside] * 10,
        scratch_shapes=[
            pltpu.SMEM(lam.shape, lam.dtype),
            vmem(xin),
            vmem(gcot),
            vmem(fcot),
            vmem(scot),
            vmem(proj),
            vmem(gw),
            vmem(vw),
            vmem(gm),
            vmem(gs),
            vmem(vm),
            vmem(vs),
            pltpu.VMEM((nfs, pieces, part, cols), bf16),
            pltpu.VMEM((rank, cols), f32),
            pltpu.VMEM((depth, cols), f32),
            pltpu.VMEM((nx, nz, share, cols), bf16),
            pltpu.VMEM((nx, nz, share, cols), bf16),
            pltpu.VMEM((nz, share, cols), bf16),
            pltpu.VMEM((nz, share, cols), bf16),
            pltpu.VMEM((nfs, share, cols), bf16),
            pltpu.VMEM((rank, cols), f32),
            pltpu.VMEM((nt, 2, 8, 128), f32),
            dma((8,)),
            dma((4, CHUNKS)),
            dma((2, nz, items)),
            dma((nz, items)),
            dma((nx, nz, pieces)),
            dma((nx, nz, pieces)),
            dma((nx,)),
            dma((nx,)),
            dma((nz,)),
            dma((nz,)),
            dma((nz,)),
            dma((nz,)),
            dma((nx, nz)),
            dma((nx, nz)),
            dma((nt,)),
            dma((nt,)),
        ],
        compiler_params=pltpu.CompilerParams(
            collective_id=0, has_side_effects=True, vmem_limit_bytes=40 * 1024 * 1024
        ),
    )(*arrays)
    return tuple(
        pl.pallas_call(
            put_kernel,
            out_shape=results,
            in_specs=[inside] * 10,
            out_specs=[anywhere] * 10,
            scratch_shapes=[dma((10,))],
            compiler_params=pltpu.CompilerParams(vmem_limit_bytes=8 * 1024 * 1024),
        )(*held)
    )


def solution(mesh):
    nz, nx = factor_fs(mesh.shape["fs"])
    split, whole = P("fs", "tp"), P(None, "tp")
    placed = (P("fs", None), split, split, split, P("tp"), P()) + (split,) * 6
    return jax.shard_map(
        functools.partial(per_device, nz, nx, mesh.shape["tp"]),
        mesh=mesh,
        in_specs=placed,
        out_specs=(split, split, whole, split, split, split, split, whole, split, split),
        check_vma=False,
    )
```

```python
import functools

import jax
import jax.numpy as jnp
from jax import lax
from jax.experimental import pallas as pl
from jax.experimental.pallas import tpu as pltpu
from jax.sharding import PartitionSpec as P

VDIM = 128
PIECES = 8
PIECE_ROWS = 16
CROSS_END = 1
CROSS_INNER = 2
CHUNKS = 4
DEPTH = 3
HOLD_X = 5
R1A = 2
R1B = 5
R2A = 4
R3A = 2

moment_decay = 0.9
square_decay = 0.95
adam_floor = 1e-08
learn_rate = 0.02
rms_floor = 0.1

MESH = pl.DeviceIdType.MESH
f32, bf16 = jnp.float32, jnp.bfloat16


def factor_fs(count):
    inner = 1
    while (2 * inner) ** 2 <= count and count % (2 * inner) == 0:
        inner *= 2
    return count // inner, inner


def kernel(
    nz,
    nx,
    nt,
    x_hbm,
    gcot_hbm,
    fcot_hbm,
    scot_hbm,
    lam_hbm,
    proj_hbm,
    gw_hbm,
    gm_hbm,
    gs_hbm,
    vw_hbm,
    vm_hbm,
    vs_hbm,
    new_gw,
    gsteps,
    gcopy,
    new_gm,
    new_gs,
    new_vw,
    vsteps,
    vcopy,
    new_vm,
    new_vs,
    lam_ref,
    xv,
    gcv,
    fcv,
    scv,
    pv,
    gw,
    vw,
    gm,
    gs,
    vm,
    vs,
    wall,
    proj_t,
    acc,
    updates,
    rsrc,
    rsx,
    zsrc,
    rsz,
    dall,
    dcat,
    sums,
    in_sem,
    x_sem,
    wz_send,
    wz_recv,
    wx_send,
    wx_recv,
    rx_send,
    rx_recv,
    rz_send,
    rz_recv,
    dz_send,
    dz_recv,
    dx_send,
    dx_recv,
    t_send,
    t_recv,
):
    nfs = nz * nx
    f = lax.axis_index("fs")
    t = lax.axis_index("tp")
    z = lax.div(f, nx)
    x = lax.rem(f, nx)
    rows, cg = gw.shape
    cv = vw.shape[1]
    cols = cg + cv
    rank = acc.shape[0]
    share = rank // nfs
    pieces, part = wall.shape[1:3]
    tokens = x_hbm.shape[0] // CHUNKS
    cross_end = pieces * CROSS_END // PIECES
    cross_inner = pieces * CROSS_INNER // PIECES
    items = [(k, p) for k in range(nx) for p in range(pieces)]

    def zpeer(k):
        return lax.rem(z + k, nz)

    def xpeer(k):
        return lax.rem(x + k, nx)

    barrier = pltpu.get_barrier_semaphore()
    for k in range(1, nz):
        pl.semaphore_signal(barrier, inc=1, device_id=(zpeer(k) * nx + x, t), device_id_type=MESH)
    for k in range(1, nx):
        pl.semaphore_signal(barrier, inc=1, device_id=(z * nx + xpeer(k), t), device_id_type=MESH)
    for k in range(1, nt):
        pl.semaphore_signal(barrier, inc=1, device_id=(f, lax.rem(t + k, nt)), device_id_type=MESH)

    small = [
        pltpu.make_async_copy(src, dst, in_sem.at[i])
        for i, (src, dst) in enumerate(
            [
                (gw_hbm, gw),
                (vw_hbm, vw),
                (proj_hbm, pv),
                (gm_hbm, gm),
                (gs_hbm, gs),
                (vm_hbm, vm),
                (vs_hbm, vs),
                (lam_hbm, lam_ref),
            ]
        )
        if src is not lam_hbm or cv > VDIM
    ]
    if cv == VDIM:
        lam_ref = lam_hbm

    def chunk_copies(c):
        at = pl.ds(c * tokens, tokens)
        return [
            pltpu.make_async_copy(src.at[at], dst.at[at], x_sem.at[i, c])
            for i, (src, dst) in enumerate(
                [(x_hbm, xv), (gcot_hbm, gcv), (fcot_hbm, fcv), (scot_hbm, scv)]
            )
        ]

    for copy in small[:3] + small[7:] + chunk_copies(0):
        copy.start()
    small[0].wait()
    small[1].wait()
    for c in range(1, DEPTH):
        for copy in chunk_copies(c):
            copy.start()
    for p in range(pieces):
        at = pl.ds(p * part, part)
        wall[f, p, :, :cg] = gw[at, :].astype(bf16)
        wall[f, p, :, cg:] = vw[at, :].astype(bf16)

    def valid(row):
        return jnp.logical_and(row >= 0, row < nz)

    def at_end(row):
        return jnp.logical_or(row == 0, row == nz - 1)

    def crosses(p, row):
        return jnp.logical_or(p < cross_end, jnp.logical_and(p < cross_inner, jnp.logical_not(at_end(row))))

    def wz(way, src_z, k, p, peer):
        owner = src_z * nx + xpeer(k)
        return pltpu.make_async_remote_copy(
            src_ref=wall.at[owner, p],
            dst_ref=wall.at[owner, p],
            send_sem=wz_send.at[(way + 1) // 2, src_z, k],
            recv_sem=wz_recv.at[src_z, k, p] if isinstance(p, int) else wz_recv.at[src_z, k, 0],
            device_id=(peer * nx + x, t),
            device_id_type=MESH,
        )

    def wx(k, p, src_z, src_x):
        owner = src_z * nx + src_x
        return pltpu.make_async_remote_copy(
            src_ref=wall.at[owner, p],
            dst_ref=wall.at[owner, p],
            send_sem=wx_send.at[k, src_z],
            recv_sem=wx_recv.at[src_x, src_z, p] if isinstance(p, int) else wx_recv.at[src_x, src_z, 0],
            device_id=(z * nx + xpeer(k), t),
            device_id_type=MESH,
        )

    def along(src_z, k, p):
        for way in (1, -1):

            @pl.when(valid(z + way))
            def _():
                wz(way, src_z, k, p, z + way).start()

    def over(src_z, p):
        for k in range(1, nx):
            wx(k, p, src_z, x).start()

    def rides(step, p, src_z):
        here = crosses(p, src_z)
        return jnp.logical_or(here, at_end(src_z)) if step < 2 else here

    def relay(step, k, p):
        for way in (1, -1):
            src_z = z - way * step

            @pl.when(jnp.logical_and(valid(src_z), rides(step, p, src_z) if k else True))
            def _():
                wz(way, src_z, k, p, z - way).wait_recv()

                @pl.when(jnp.logical_and(valid(z + way), crosses(p, src_z) if k else True))
                def _():
                    wz(way, src_z, k, p, z + way).start()

                if not k:

                    @pl.when(jnp.logical_not(rides(step, p, src_z)))
                    def _():
                        over(src_z, p)

    def relays(step, others, lo, hi):
        if step < nz:
            for p in range(min(lo, pieces), min(hi, pieces)):
                for k in range(1, nx) if others else (0,):
                    relay(step, k, p)

    def turns(lo, hi):
        for p in range(min(lo, pieces), min(hi, pieces)):
            for k in range(1, nx):
                wx(k, p, z, xpeer(k)).wait_recv()

                @pl.when(rides(0, p, z))
                def _():
                    along(z, k, p)

    def sent(step):
        for way in (1, -1) if step else (0,):
            src_z = z - way * step
            end = at_end(src_z)
            for go in (way,) if step else (1, -1):
                onward = jnp.logical_and(valid(src_z), valid(z + go))

                @pl.when(onward)
                def _():
                    wz(go, src_z, 0, pl.ds(0, pieces), z + go).wait_send()

                for count, case in (
                    (cross_end if step else pieces, end),
                    (cross_inner, jnp.logical_not(end)),
                ):
                    if count:

                        @pl.when(jnp.logical_and(onward, case))
                        def _():
                            for k in range(1, nx):
                                wz(go, src_z, k, pl.ds(0, count), z + go).wait_send()

            for first, case in ((cross_end, end), (cross_inner, jnp.logical_not(end))):
                if step == 1 and first == cross_end and case is end:
                    continue
                if not step:
                    first = 0

                @pl.when(jnp.logical_and(valid(src_z), case))
                def _():
                    for k in range(1, nx):
                        wx(k, pl.ds(first, pieces - first), src_z, x).wait_send()

    pl.semaphore_wait(barrier, (nz - 1) + (nx - 1) + (nt - 1))
    for p in range(pieces):
        along(z, 0, p)
        if p < HOLD_X:
            over(z, p)

    for copy in small[2:3] + small[7:]:
        copy.wait()
    proj_t[...] = pv[...].T
    head = lax.broadcasted_iota(jnp.int32, (1, cv), 1) // VDIM
    lam = jnp.zeros((1, cv), f32)
    for h in range(cv // VDIM):
        lam = jnp.where(head == h, lam_ref[h], lam)
    for c in range(CHUNKS):
        for copy in chunk_copies(c):
            copy.wait()

        if c + DEPTH < CHUNKS:
            for copy in chunk_copies(c + DEPTH):
                copy.start()
        elif c + DEPTH == CHUNKS:
            for i in range(3, 7):
                small[i].start()
        at = pl.ds(c * tokens, tokens)
        upper = lax.dot_general(
            proj_t[...], xv[at, :], (((1,), (1,)), ((), ())), preferred_element_type=f32
        ).astype(bf16)
        value = (fcv[at, :].astype(f32) - lam * scv[at, :].astype(f32)).astype(bf16)
        gate_part = jnp.dot(upper, gcv[at, :], preferred_element_type=f32)
        value_part = jnp.dot(upper, value, preferred_element_type=f32)
        if c:
            gate_part += acc[:, :cg]
            value_part += acc[:, cg:]
        acc[:, :cg] = gate_part
        acc[:, cg:] = value_part

    for zi in range(nz):
        for xi in range(nx):
            at = pl.ds((zi * nx + xi) * share, share)
            rsrc[xi, zi] = acc[at, :].astype(bf16)

    def rx(k, zi, src_x, dst_x):
        return pltpu.make_async_remote_copy(
            src_ref=rsrc.at[dst_x, zi],
            dst_ref=rsx.at[src_x, zi],
            send_sem=rx_send.at[k, zi],
            recv_sem=rx_recv.at[src_x, zi],
            device_id=(z * nx + xpeer(k), t),
            device_id_type=MESH,
        )

    def rz(k, src_z, dst_z):
        return pltpu.make_async_remote_copy(
            src_ref=zsrc.at[dst_z],
            dst_ref=rsz.at[src_z],
            send_sem=rz_send.at[k],
            recv_sem=rz_recv.at[src_z],
            device_id=(zpeer(k) * nx + x, t),
            device_id_type=MESH,
        )

    def column_sum(zi):
        at = pl.ds(pl.multiple_of((zi * nx + x) * share, share), share)
        total = acc[at, :]
        for k in range(1, nx):
            rx(k, zi, xpeer(k), x).wait_recv()
            total = total + rsx[xpeer(k), zi].astype(f32)
        return total

    far = list(range(1, nz))
    for j in far + [0]:
        for k in range(1, nx):
            rx(k, zpeer(j), x, xpeer(k)).start()
    for p in range(min(HOLD_X, pieces), pieces):
        over(z, p)
    relays(1, 0, 0, R1A)
    turns(0, R1A)
    for j in far:
        zsrc[zpeer(j)] = column_sum(zpeer(j)).astype(bf16)
        rz(j, z, zpeer(j)).start()
    relays(1, 0, R1A, R1B)
    turns(R1A, R1B)
    for i in range(3, 7):
        small[i].wait()
    low = column_sum(z)
    for k in range(1, nz):
        rz(k, zpeer(k), z).wait_recv()
        low = low + rsz[zpeer(k)].astype(f32)

    for first, second, new_m, new_s, at in (
        (gm, gs, new_gm, new_gs, slice(0, cg)),
        (vm, vs, new_vm, new_vs, slice(cg, cols)),
    ):
        mine = low[:, at]
        new_first = moment_decay * first[...] + (1.0 - moment_decay) * mine
        new_second = square_decay * second[...] + (1.0 - square_decay) * mine * mine
        new_m[...] = new_first
        new_s[...] = new_second
        dall[f, :, at] = (new_first / (jnp.sqrt(new_second) + adam_floor)).astype(bf16)

    def dz(k, src_z):
        owner = src_z * nx + x
        return pltpu.make_async_remote_copy(
            src_ref=dall.at[owner],
            dst_ref=dall.at[owner],
            send_sem=dz_send.at[k],
            recv_sem=dz_recv.at[src_z],
            device_id=(zpeer(k) * nx + x, t),
            device_id_type=MESH,
        )

    def dx(k, src_z, src_x):
        owner = src_z * nx + src_x
        return pltpu.make_async_remote_copy(
            src_ref=dall.at[owner],
            dst_ref=dall.at[owner],
            send_sem=dx_send.at[k, src_z],
            recv_sem=dx_recv.at[src_x, src_z],
            device_id=(z * nx + xpeer(k), t),
            device_id_type=MESH,
        )

    for k in range(1, nz):
        dz(k, z).start()
    for m in range(1, nx):
        dx(m, z, x).start()
    relays(1, 0, R1B, pieces)
    turns(R1B, pieces)
    relays(1, 1, 0, cross_inner)
    relays(2, 0, 0, R2A)
    for k in range(1, nz):
        dz(k, zpeer(k)).wait_recv()
        for m in range(1, nx):
            dx(m, zpeer(k), x).start()
    relays(2, 0, R2A, pieces)
    relays(2, 1, 0, cross_inner)
    relays(3, 0, 0, R3A)
    for m in range(1, nx):
        for zi in range(nz):
            dx(m, zi, xpeer(m)).wait_recv()

    for j in range(nfs):
        dcat[pl.ds(j * share, share), :] = dall[j].astype(f32)
    direction = dcat[...].astype(bf16)

    def expand(j, squares):
        at = pl.ds(pl.multiple_of(j * rows, rows), rows)
        block = jnp.dot(pv[at, :], direction, preferred_element_type=f32)
        updates[at, :] = block
        return squares + jnp.sum((block * block).reshape(rows // 8, 8, cols), axis=0)

    squares = lax.fori_loop(0, nfs, expand, jnp.zeros((8, cols), f32))
    squares = jnp.sum(squares, axis=0, keepdims=True)
    gate_sum = jnp.sum(squares[:, :cg], axis=1, keepdims=True)
    value_sum = jnp.sum(squares[:, cg:], axis=1, keepdims=True)
    sums[t, 0] = jnp.broadcast_to(gate_sum, (8, 128))
    sums[t, 1] = jnp.broadcast_to(value_sum, (8, 128))

    def tp(k, src_t):
        return pltpu.make_async_remote_copy(
            src_ref=sums.at[src_t],
            dst_ref=sums.at[src_t],
            send_sem=t_send.at[k],
            recv_sem=t_recv.at[src_t],
            device_id=(f, lax.rem(t + k, nt)),
            device_id_type=MESH,
        )

    for k in range(1, nt):
        tp(k, t).start()
    relays(3, 0, R3A, pieces)
    relays(3, 1, 0, cross_inner)
    for step in range(4, nz):
        relays(step, 0, 0, pieces)
        relays(step, 1, 0, cross_inner)
    relays(1, 1, cross_inner, pieces)
    for k in range(1, nt):
        tp(k, lax.rem(t + k, nt)).wait_recv()
    whole = sums[0]
    for k in range(1, nt):
        whole = whole + sums[k]
    entries = nfs * rows * nt
    gscale = (1.0 / (jnp.sqrt(whole[0] / (entries * cg)) + rms_floor))[0:1, 0:1]
    vscale = (1.0 / (jnp.sqrt(whole[1] / (entries * cv)) + rms_floor))[0:1, 0:1]

    at = pl.ds(pl.multiple_of(f * rows, rows), rows)
    gstep = updates[at, :cg] * gscale
    vstep = updates[at, cg:] * vscale
    gsteps[...] = gstep
    vsteps[...] = vstep
    new_gw[...] = gw[...] - learn_rate * gstep
    new_vw[...] = vw[...] - learn_rate * vstep

    def finish(j, p):
        at = pl.ds(pl.multiple_of(j * rows + p * part, part), part)
        held = wall[j, p].astype(f32)
        update = updates[at, :]
        gcopy[at, :] = (held[:, :cg] - learn_rate * (update[:, :cg] * gscale)).astype(bf16)
        vcopy[at, :] = (held[:, cg:] - learn_rate * (update[:, cg:] * vscale)).astype(bf16)

    def finish_block(j, lo, hi):
        def body(p, carry):
            finish(j, p)
            return carry

        lax.fori_loop(lo, hi, body, 0)

    for zi in range(nz):
        finish_block(zi * nx + x, 0, pieces)
        for k in range(1, nx):
            finish_block(zi * nx + xpeer(k), 0, cross_end)
    for k in range(1, nx):
        finish_block(z * nx + xpeer(k), cross_end, pieces)
    for k in range(1, nz):
        rz(k, z, zpeer(k)).wait_send()
        dz(k, z).wait_send()
    for m in range(1, nx):
        for zi in range(nz):
            dx(m, zi, x).wait_send()
            rx(m, zi, x, xpeer(m)).wait_send()
    for k in range(1, nt):
        tp(k, t).wait_send()
    for step in range(max(nz - 1, 1)):
        sent(step)
    for step in range(1, nz):
        for p in range(cross_end, pieces):
            for way in (1, -1):
                src_z = z - way * step

                @pl.when(valid(src_z))
                def _():
                    for k in range(1, nx):

                        @pl.when(jnp.logical_not(rides(step, p, src_z)))
                        def _():
                            wx(k, p, src_z, xpeer(k)).wait_recv()

                        finish(src_z * nx + xpeer(k), p)

    if nz > 1:
        sent(nz - 1)


def put_kernel(*refs):
    count = (len(refs) - 1) // 2
    sem = refs[-1]
    copies = [pltpu.make_async_copy(refs[i], refs[count + i], sem.at[i]) for i in range(count)]
    for copy in copies:
        copy.start()
    for copy in copies:
        copy.wait()


def per_device(nz, nx, nt, xin, gcot, fcot, scot, lam, proj, gw, gm, gs, vw, vm, vs):
    nfs = nz * nx
    rows, cg = gw.shape
    cv = vw.shape[1]
    cols = cg + cv
    depth, rank = proj.shape
    share = rank // nfs
    pieces = min(PIECES, rows // PIECE_ROWS)
    part = rows // pieces
    dma = pltpu.SemaphoreType.DMA
    shape = jax.ShapeDtypeStruct
    vmem = lambda a: pltpu.VMEM(a.shape, a.dtype)
    results = [
        shape((rows, cg), f32),
        shape((rows, cg), f32),
        shape((depth, cg), bf16),
        shape(gm.shape, f32),
        shape(gs.shape, f32),
        shape((rows, cv), f32),
        shape((rows, cv), f32),
        shape((depth, cv), bf16),
        shape(vm.shape, f32),
        shape(vs.shape, f32),
    ]
    arrays = [xin, gcot, fcot, scot, lam, proj, gw, gm, gs, vw, vm, vs]
    alone = cv == VDIM
    arrays = [
        a if alone and a is lam else pltpu.with_memory_space_constraint(a, pltpu.HBM)
        for a in arrays
    ]
    anywhere = pl.BlockSpec(memory_space=pl.ANY)
    inside = pl.BlockSpec(memory_space=pltpu.VMEM)
    held = pl.pallas_call(
        functools.partial(kernel, nz, nx, nt),
        out_shape=[vmem(a) for a in results],
        in_specs=[
            pl.BlockSpec(memory_space=pltpu.SMEM) if alone and a is lam else anywhere
            for a in (xin, gcot, fcot, scot, lam, proj, gw, gm, gs, vw, vm, vs)
        ],
        out_specs=[inside] * 10,
        scratch_shapes=[
            pltpu.SMEM(lam.shape, lam.dtype),
            vmem(xin),
            vmem(gcot),
            vmem(fcot),
            vmem(scot),
            vmem(proj),
            vmem(gw),
            vmem(vw),
            vmem(gm),
            vmem(gs),
            vmem(vm),
            vmem(vs),
            pltpu.VMEM((nfs, pieces, part, cols), bf16),
            pltpu.VMEM((rank, depth), bf16),
            pltpu.VMEM((rank, cols), f32),
            pltpu.VMEM((depth, cols), f32),
            pltpu.VMEM((nx, nz, share, cols), bf16),
            pltpu.VMEM((nx, nz, share, cols), bf16),
            pltpu.VMEM((nz, share, cols), bf16),
            pltpu.VMEM((nz, share, cols), bf16),
            pltpu.VMEM((nfs, share, cols), bf16),
            pltpu.VMEM((rank, cols), f32),
            pltpu.VMEM((nt, 2, 8, 128), f32),
            dma((8,)),
            dma((4, CHUNKS)),
            dma((2, nz, nx)),
            dma((nz, nx, pieces)),
            dma((nx, nz)),
            dma((nx, nz, pieces)),
            dma((nx, nz)),
            dma((nx, nz)),
            dma((nz,)),
            dma((nz,)),
            dma((nz,)),
            dma((nz,)),
            dma((nx, nz)),
            dma((nx, nz)),
            dma((nt,)),
            dma((nt,)),
        ],
        compiler_params=pltpu.CompilerParams(
            collective_id=0, has_side_effects=True, vmem_limit_bytes=40 * 1024 * 1024
        ),
    )(*arrays)
    return tuple(
        pl.pallas_call(
            put_kernel,
            out_shape=results,
            in_specs=[inside] * 10,
            out_specs=[anywhere] * 10,
            scratch_shapes=[dma((10,))],
            compiler_params=pltpu.CompilerParams(vmem_limit_bytes=8 * 1024 * 1024),
        )(*held)
    )


def solution(mesh):
    nz, nx = factor_fs(mesh.shape["fs"])
    split, whole = P("fs", "tp"), P(None, "tp")
    placed = (P("fs", None), split, split, split, P("tp"), P()) + (split,) * 6
    return jax.shard_map(
        functools.partial(per_device, nz, nx, mesh.shape["tp"]),
        mesh=mesh,
        in_specs=placed,
        out_specs=(split, split, whole, split, split, split, split, whole, split, split),
        check_vma=False,
    )
```

```python
import functools

import jax
import jax.numpy as jnp
from jax import lax
from jax.experimental import pallas as pl
from jax.experimental.pallas import tpu as pltpu
from jax.sharding import PartitionSpec as P

VDIM = 128
PIECES = 8
PIECE_ROWS = 16
CROSS_END = 1
CROSS_INNER = 1
CHUNKS = 4
DEPTH = 3
SINGLES = 2
HOLD_X = 5
HOLD_Z = 5
FIRST_A = (0, 5, 0, 4)
FIRST_B = (5, 8, 4, 6)
FIRST_C = (8, 8, 6, 8)
SECOND_A = (0, 7, 0, 3)
SECOND_B = (7, 8, 3, 8)
THIRD_A = (0, 4, 0, 4)
THIRD_B = (4, 6, 4, 6)
THIRD_C = (6, 8, 6, 8)

moment_decay = 0.9
square_decay = 0.95
adam_floor = 1e-08
learn_rate = 0.02
rms_floor = 0.1

MESH = pl.DeviceIdType.MESH
f32, bf16 = jnp.float32, jnp.bfloat16


def factor_fs(count):
    inner = 1
    while (2 * inner) ** 2 <= count and count % (2 * inner) == 0:
        inner *= 2
    return count // inner, inner


def kernel(
    nz,
    nx,
    nt,
    x_hbm,
    gcot_hbm,
    fcot_hbm,
    scot_hbm,
    lam_hbm,
    proj_hbm,
    gw_hbm,
    gm_hbm,
    gs_hbm,
    vw_hbm,
    vm_hbm,
    vs_hbm,
    new_gw,
    gsteps,
    gcopy,
    new_gm,
    new_gs,
    new_vw,
    vsteps,
    vcopy,
    new_vm,
    new_vs,
    lam_ref,
    xv,
    gcv,
    fcv,
    scv,
    pv,
    gw,
    vw,
    gm,
    gs,
    vm,
    vs,
    wall,
    proj_t,
    gram_high,
    gram_low,
    acc,
    updates,
    rsrc,
    rsx,
    zsrc,
    rsz,
    handed,
    low,
    dall,
    dcat,
    sums,
    in_sem,
    x_sem,
    wz_send,
    wz_recv,
    wz_more,
    wx_send,
    wx_recv,
    wx_own,
    rx_send,
    rx_recv,
    rz_send,
    rz_recv,
    dz_send,
    dz_recv,
    dx_send,
    dx_recv,
    t_send,
    t_recv,
    far_sem,
    hand_send,
    hand_recv,
):
    nfs = nz * nx
    f = lax.axis_index("fs")
    t = lax.axis_index("tp")
    z = lax.div(f, nx)
    x = lax.rem(f, nx)
    rows, cg = gw.shape
    cv = vw.shape[1]
    cols = cg + cv
    rank = acc.shape[0]
    share = rank // nfs
    part = wall.shape[1]
    pieces = rows // part
    tokens = x_hbm.shape[0] // CHUNKS
    cross_end = pieces * CROSS_END // PIECES
    cross_inner = pieces * CROSS_INNER // PIECES
    items = [(k, p) for k in range(nx) for p in range(pieces)]

    def zpeer(k):
        return lax.rem(z + k, nz)

    def xpeer(k):
        return lax.rem(x + k, nx)

    def valid(row):
        return jnp.logical_and(row >= 0, row < nz)

    barrier = pltpu.get_barrier_semaphore()
    for way in (1, -1):

        @pl.when(valid(z + way))
        def _():
            pl.semaphore_signal(barrier, inc=1, device_id=((z + way) * nx + x, t), device_id_type=MESH)

    for k in range(1, nx):
        pl.semaphore_signal(barrier, inc=1, device_id=(z * nx + xpeer(k), t), device_id_type=MESH)
    for k in range(1, nt):
        pl.semaphore_signal(barrier, inc=1, device_id=(f, lax.rem(t + k, nt)), device_id_type=MESH)

    small = [
        pltpu.make_async_copy(src, dst, in_sem.at[i])
        for i, (src, dst) in enumerate(
            [
                (gw_hbm, gw),
                (vw_hbm, vw),
                (proj_hbm, pv),
                (gm_hbm, gm),
                (gs_hbm, gs),
                (vm_hbm, vm),
                (vs_hbm, vs),
                (lam_hbm, lam_ref),
            ]
        )
        if src is not lam_hbm or cv > VDIM
    ]
    if cv == VDIM:
        lam_ref = lam_hbm

    def chunk_copies(c):
        at = pl.ds(c * tokens, tokens)
        return [
            pltpu.make_async_copy(src.at[at], dst.at[at], x_sem.at[i, c % DEPTH])
            for i, (src, dst) in enumerate(
                [(x_hbm, xv), (gcot_hbm, gcv), (fcot_hbm, fcv), (scot_hbm, scv)]
            )
        ]

    for copy in small[:3] + small[7:] + chunk_copies(0):
        copy.start()
    small[0].wait()
    small[1].wait()
    for c in range(1, DEPTH):
        for copy in chunk_copies(c):
            copy.start()
    for p in range(pieces):
        at = pl.ds(p * part, part)
        wall[f * pieces + p, :, :cg] = gw[at, :].astype(bf16)
        wall[f * pieces + p, :, cg:] = vw[at, :].astype(bf16)

    def at_end(row):
        return jnp.logical_or(row == 0, row == nz - 1)

    def crosses(p, row):
        return jnp.logical_or(p < cross_end, jnp.logical_and(p < cross_inner, jnp.logical_not(at_end(row))))

    def wz(way, src_z, k, p, peer, here=False):
        at = (src_z * nx + xpeer(k)) * pieces + p
        away = lax.rem(src_z - (z if here else peer) + nz, nz) - 1
        if k and p >= cross_inner:
            sem = wz_recv.at[away, pieces]
        elif k:
            sem = wz_more.at[away, (k - 1) * max(cross_inner, 1) + p]
        else:
            sem = wz_recv.at[away, p]
        return pltpu.make_async_remote_copy(
            src_ref=wall.at[at],
            dst_ref=wall.at[at],
            send_sem=wz_send.at[(way + 1) // 2, src_z],
            recv_sem=sem,
            device_id=(peer * nx + x, t),
            device_id_type=MESH,
        )

    def wx(k, p, src_z, src_x, own):
        at = (src_z * nx + src_x) * pieces + p
        if own:
            sem = wx_own.at[nx - k - 1, p]
        else:
            sem = wx_recv.at[nx - k - 1, lax.rem(src_z - z + nz, nz) - 1, group_of(p)]
        return pltpu.make_async_remote_copy(
            src_ref=wall.at[at],
            dst_ref=wall.at[at],
            send_sem=wx_send.at[k - 1, src_z],
            recv_sem=sem,
            device_id=(z * nx + xpeer(k), t),
            device_id_type=MESH,
        )

    def group_of(p):
        return max(p - (pieces - SINGLES) + 1, 0)

    def await_sent(sem, count):
        pieces_of = wall.at[pl.ds(0, count)]
        pltpu.make_async_remote_copy(
            src_ref=pieces_of,
            dst_ref=pieces_of,
            send_sem=sem,
            recv_sem=sem,
            device_id=(z * nx + xpeer(1), t),
            device_id_type=MESH,
        ).wait_send()

    def await_got(sem, ref):
        pltpu.make_async_remote_copy(
            src_ref=ref,
            dst_ref=ref,
            send_sem=sem,
            recv_sem=sem,
            device_id=(z * nx + xpeer(1), t),
            device_id_type=MESH,
        ).wait_recv()

    def along(src_z, k, p):
        for way in (1, -1):

            @pl.when(valid(z + way))
            def _():
                wz(way, src_z, k, p, z + way).start()

    def over(src_z, p, own=False):
        for k in range(1, nx):
            wx(k, p, src_z, x, own).start()

    def rides(step, p, src_z):
        here = crosses(p, src_z)
        return jnp.logical_or(here, at_end(src_z)) if step < 2 else here

    def relay(step, k, p, where):
        for way in (1, -1):
            src_z = z - way * step
            come = jnp.logical_and(valid(src_z), where)
            if k:
                come = jnp.logical_and(come, crosses(p, src_z))

            @pl.when(come)
            def _():
                wz(way, src_z, k, p, z - way, True).wait_recv()

                @pl.when(valid(z + way))
                def _():
                    wz(way, src_z, k, p, z + way).start()

                if not k:

                    @pl.when(jnp.logical_not(rides(step, p, src_z)))
                    def _():
                        over(src_z, p)

    def relays(step, lo_end, hi_end, lo, hi):
        if step < nz:
            for p in range(pieces):
                ends, rest = lo_end <= p < hi_end, lo <= p < hi
                if ends or rest:
                    where = True if ends and rest else end if ends else jnp.logical_not(end)
                    relay(step, 0, p, where)

    def relay_others(step, where):
        if step < nz:
            for p in range(cross_inner):
                for k in range(1, nx):
                    relay(step, k, p, where)

    def turns(lo, hi):
        for p in range(min(lo, pieces), min(hi, pieces)):
            for k in range(1, nx):
                await_got(wx_own.at[k - 1, p], wall.at[p])

                @pl.when(rides(0, p, z))
                def _():
                    along(z, k, p)

    def sent(step):
        for way in (1, -1) if step else (0,):
            src_z = z - way * step
            src_end = at_end(src_z)
            for case, many, crossing, passed in (
                (src_end, cross_end if step else pieces, cross_end, step == 1),
                (jnp.logical_not(src_end), cross_inner, cross_inner, False),
            ):

                @pl.when(jnp.logical_and(valid(src_z), case))
                def _():
                    for go in (way,) if step else (1, -1):

                        @pl.when(valid(z + go))
                        def _():
                            await_sent(wz_send.at[(go + 1) // 2, src_z], pieces + (nx - 1) * many)

                    if not passed:
                        for k in range(1, nx):
                            await_sent(wx_send.at[k - 1, src_z], pieces - crossing if step else pieces)

    end = at_end(z)
    next_rows = jnp.where(valid(z + 1), 1, 0) + jnp.where(valid(z - 1), 1, 0)

    def tell(i):
        if i < nz - 2:
            for way in (1, -1):

                @pl.when(valid(z + way))
                def _():
                    pl.semaphore_signal(
                        far_sem.at[i], inc=1, device_id=((z + way) * nx + x, t), device_id_type=MESH
                    )

    def hear(i):
        if i < nz - 2:
            pl.semaphore_wait(far_sem.at[i], next_rows)

    pl.semaphore_wait(barrier, next_rows + (nx - 1) + (nt - 1))
    tell(0)
    for p in range(pieces):
        if p < HOLD_Z:
            along(z, 0, p)
        else:

            @pl.when(jnp.logical_not(end))
            def _():
                along(z, 0, p)

        if p < HOLD_X:
            over(z, p, True)

    for copy in small[2:3] + small[7:]:
        copy.wait()
    proj_t[...] = pv[...].T
    head = lax.broadcasted_iota(jnp.int32, (1, cv), 1) // VDIM
    lam = jnp.zeros((1, cv), f32)
    for h in range(cv // VDIM):
        lam = jnp.where(head == h, lam_ref[h], lam)
    for c in range(CHUNKS):
        for copy in chunk_copies(c):
            copy.wait()

        if c + DEPTH < CHUNKS:
            for copy in chunk_copies(c + DEPTH):
                copy.start()
        elif c + DEPTH == CHUNKS:
            for i in range(3, 7):
                small[i].start()
        at = pl.ds(c * tokens, tokens)
        upper = lax.dot_general(
            proj_t[...], xv[at, :], (((1,), (1,)), ((), ())), preferred_element_type=f32
        ).astype(bf16)
        value = (fcv[at, :].astype(f32) - lam * scv[at, :].astype(f32)).astype(bf16)
        gate_part = jnp.dot(upper, gcv[at, :], preferred_element_type=f32)
        value_part = jnp.dot(upper, value, preferred_element_type=f32)
        if c:
            gate_part += acc[:, :cg]
            value_part += acc[:, cg:]
        acc[:, :cg] = gate_part
        acc[:, cg:] = value_part
        if c % 2:
            hear(c // 2)
            tell(c // 2 + 1)

    for i in range(CHUNKS // 2, nz - 2):
        hear(i)
        tell(i + 1)
    for zi in range(nz):
        for xi in range(nx):
            at = pl.ds((zi * nx + xi) * share, share)
            rsrc[xi, zi] = acc[at, :].astype(bf16)

    def rx(k, zi):
        return pltpu.make_async_remote_copy(
            src_ref=rsrc.at[xpeer(k), zi],
            dst_ref=rsx.at[nx - k - 1, zi],
            send_sem=rx_send.at[k - 1],
            recv_sem=rx_recv.at[nx - k - 1, zi],
            device_id=(z * nx + xpeer(k), t),
            device_id_type=MESH,
        )

    def hand(k, zi):
        row = jnp.where(z == 0, 1, nz - 2)
        return pltpu.make_async_remote_copy(
            src_ref=rsrc.at[xpeer(k), zi],
            dst_ref=handed.at[zi, (nx - k) % nx],
            send_sem=hand_send.at[0],
            recv_sem=hand_recv.at[zi],
            device_id=(row * nx + xpeer(k), t),
            device_id_type=MESH,
        )

    def rz(zi):
        return pltpu.make_async_remote_copy(
            src_ref=zsrc.at[zi],
            dst_ref=rsz.at[z - 1],
            send_sem=rz_send.at[0],
            recv_sem=rz_recv.at[0],
            device_id=(zi * nx + x, t),
            device_id_type=MESH,
        )

    far = list(range(1, nz))

    def other(j):
        return jnp.where(2 * z < nz, lax.rem(z + nz - j, nz), zpeer(j))

    def handing(j):
        return jnp.where(z == 0, nz - j, j - 1)

    inner = jnp.logical_not(end)
    beside = jnp.logical_or(z == 1, z == nz - 2)

    def row_sum(zi):
        at = pl.ds(pl.multiple_of((zi * nx + x) * share, share), share)
        low[...] = acc[at, :]
        for k in range(1, nx):
            await_got(rx_recv.at[k - 1, zi], rsx.at[0, 0])
            low[...] += rsx[k - 1, zi].astype(f32)

        @pl.when(jnp.logical_and(beside, zi != jnp.where(z == 1, 0, nz - 1)))
        def _():
            await_got(hand_recv.at[zi], handed.at[0])
            for k in range(nx):
                low[...] += handed[zi, k].astype(f32)

    @pl.when(inner)
    def _():
        for j in far:
            for k in range(1, nx):
                rx(k, other(j)).start()

    @pl.when(end)
    def _():
        for j in far:
            for k in list(range(1, nx)) + [0]:
                hand(k, handing(j)).start()

    for k in range(1, nx):
        rx(k, z).start()

    def rest_over():
        for p in range(min(HOLD_X, pieces), pieces):
            over(z, p, True)

    pl.when(end)(rest_over)

    @pl.when(end)
    def _():
        for p in range(min(HOLD_Z, pieces), pieces):
            along(z, 0, p)

    relays(1, *FIRST_A)
    gram = jnp.dot(proj_t[...], pv[...], preferred_element_type=f32)
    gram_high[...] = gram.astype(bf16)
    gram_low[...] = (gram - gram_high[...].astype(f32)).astype(bf16)

    @pl.when(inner)
    def _():
        for j in far:
            row_sum(other(j))
            zsrc[other(j)] = low[...].astype(bf16)
            rz(other(j)).start()

    pl.when(inner)(rest_over)
    relays(1, *FIRST_B)
    for i in range(3, 7):
        small[i].wait()
    row_sum(z)

    @pl.when(end)
    def _():
        await_got(rz_recv.at[0], rsz.at[pl.ds(0, nz - 2)])

    @pl.when(inner)
    def _():
        await_got(rz_recv.at[0], rsz.at[pl.ds(0, nz - 3)])

    for row in range(1, nz - 1):

        @pl.when(z != row)
        def _():
            low[...] += rsz[row - 1].astype(f32)

    for first, second, new_m, new_s, at in (
        (gm, gs, new_gm, new_gs, slice(0, cg)),
        (vm, vs, new_vm, new_vs, slice(cg, cols)),
    ):
        mine = low[:, at]
        new_first = moment_decay * first[...] + (1.0 - moment_decay) * mine
        new_second = square_decay * second[...] + (1.0 - square_decay) * mine * mine
        new_m[...] = new_first
        new_s[...] = new_second
        dall[f, :, at] = (new_first / (jnp.sqrt(new_second) + adam_floor)).astype(bf16)

    def dz(k, src_z):
        owner = src_z * nx + x
        return pltpu.make_async_remote_copy(
            src_ref=dall.at[owner],
            dst_ref=dall.at[owner],
            send_sem=dz_send.at[0],
            recv_sem=dz_recv.at[src_z],
            device_id=(zpeer(k) * nx + x, t),
            device_id_type=MESH,
        )

    def dx(k, src_z, src_x):
        owner = src_z * nx + src_x
        return pltpu.make_async_remote_copy(
            src_ref=dall.at[owner],
            dst_ref=dall.at[owner],
            send_sem=dx_send.at[k - 1],
            recv_sem=dx_recv.at[nx - k - 1],
            device_id=(z * nx + xpeer(k), t),
            device_id_type=MESH,
        )

    for k in range(1, nz):
        dz(k, z).start()
    for m in range(1, nx):
        dx(m, z, x).start()
    relays(1, *FIRST_C)
    turns(0, HOLD_X)
    relays(2, *SECOND_A)
    for k in range(1, nz):
        dz(k, zpeer(k)).wait_recv()
        for m in range(1, nx):
            dx(m, zpeer(k), x).start()
    relays(2, *SECOND_B)
    turns(HOLD_X, pieces)
    relay_others(1, jnp.logical_not(end))
    relays(3, *THIRD_A)
    for m in range(1, nx):
        await_got(dx_recv.at[m - 1], dall.at[pl.ds(0, nz)])

    for j in range(nfs):
        dcat[pl.ds(j * share, share), :] = dall[j].astype(f32)
    direction = dcat[...].astype(bf16)

    turned = jnp.dot(gram_high[...], direction, preferred_element_type=f32)
    turned += jnp.dot(gram_low[...], direction, preferred_element_type=f32)
    squares = jnp.sum((turned * dcat[...]).reshape(rank // 8, 8, cols), axis=0)
    squares = jnp.sum(squares, axis=0, keepdims=True)
    squares = jnp.maximum(squares, 0.0)
    gate_sum = jnp.sum(squares[:, :cg], axis=1, keepdims=True)
    value_sum = jnp.sum(squares[:, cg:], axis=1, keepdims=True)
    sums[t, 0] = jnp.broadcast_to(gate_sum, (8, 128))
    sums[t, 1] = jnp.broadcast_to(value_sum, (8, 128))

    def tp(k, src_t):
        return pltpu.make_async_remote_copy(
            src_ref=sums.at[src_t],
            dst_ref=sums.at[src_t],
            send_sem=t_send.at[0],
            recv_sem=t_recv.at[0],
            device_id=(f, lax.rem(t + k, nt)),
            device_id_type=MESH,
        )

    for k in range(1, nt):
        tp(k, t).start()

    def expand(j, carry):
        at = pl.ds(pl.multiple_of(j * rows, rows), rows)
        updates[at, :] = jnp.dot(pv[at, :], direction, preferred_element_type=f32)
        return carry

    relays(3, *THIRD_B)
    lax.fori_loop(0, nfs, expand, 0)
    relays(3, *THIRD_C)
    for step in range(4, nz):
        relays(step, 0, pieces, 0, pieces)
    for step in range(2, nz):
        relay_others(step, jnp.logical_not(end))
    for way in (1, -1):

        @pl.when(jnp.logical_and(valid(z - way), at_end(z - way)))
        def _():
            for p in range(cross_end, cross_inner):
                for k in range(1, nx):
                    wz(way, z - way, k, p, z - way, True).wait_recv()
            await_got(wz_recv.at[lax.rem(nz - way, nz) - 1, pieces], wall.at[pl.ds(0, (nx - 1) * (pieces - cross_inner))])

    await_got(t_recv.at[0], sums.at[pl.ds(0, nt - 1)])
    whole = sums[0]
    for k in range(1, nt):
        whole = whole + sums[k]
    entries = nfs * rows * nt
    gscale = (1.0 / (jnp.sqrt(whole[0] / (entries * cg)) + rms_floor))[0:1, 0:1]
    vscale = (1.0 / (jnp.sqrt(whole[1] / (entries * cv)) + rms_floor))[0:1, 0:1]

    at = pl.ds(pl.multiple_of(f * rows, rows), rows)
    gstep = updates[at, :cg] * gscale
    vstep = updates[at, cg:] * vscale
    gsteps[...] = gstep
    vsteps[...] = vstep
    new_gw[...] = gw[...] - learn_rate * gstep
    new_vw[...] = vw[...] - learn_rate * vstep

    def finish(j, p):
        at = pl.ds(pl.multiple_of(j * rows + p * part, part), part)
        held = wall[j * pieces + p].astype(f32)
        update = updates[at, :]
        gcopy[at, :] = (held[:, :cg] - learn_rate * (update[:, :cg] * gscale)).astype(bf16)
        vcopy[at, :] = (held[:, cg:] - learn_rate * (update[:, cg:] * vscale)).astype(bf16)

    def finish_block(j, lo, hi):
        def body(p, carry):
            finish(j, p)
            return carry

        lax.fori_loop(lo, hi, body, 0)

    for zi in range(nz):
        finish_block(zi * nx + x, 0, pieces)
    for k in range(1, nx):
        finish_block(z * nx + xpeer(k), 0, pieces)

    @pl.when(inner)
    def _():
        await_got(rz_send.at[0], zsrc.at[pl.ds(0, nz - 1)])
        for m in range(1, nx):
            await_got(rx_send.at[m - 1], rsrc.at[0])

    @pl.when(end)
    def _():
        await_got(hand_send.at[0], handed.at[pl.ds(0, nz - 1)])
        for m in range(1, nx):
            await_got(rx_send.at[m - 1], rsrc.at[0, 0])

    await_got(dz_send.at[0], dall.at[pl.ds(0, nz - 1)])
    for m in range(1, nx):
        await_got(dx_send.at[m - 1], dall.at[pl.ds(0, nz)])
    await_got(t_send.at[0], sums.at[pl.ds(0, nt - 1)])
    for step in range(max(nz - 1, 1)):
        sent(step)
    for step in range(1, nz):
        relay_others(step, end)
    if cross_end:
        for zi in range(1, nz):
            for k in range(1, nx):
                finish_block(zpeer(zi) * nx + xpeer(k), 0, cross_end)
    for step in range(1, nz):
        for p in range(cross_end, pieces):
            for way in (1, -1):
                src_z = z - way * step

                @pl.when(valid(src_z))
                def _():
                    for k in range(1, nx):
                        group = group_of(p)
                        whole_row = jnp.logical_not(at_end(src_z))
                        sem = wx_recv.at[k - 1, lax.rem(src_z - z + nz, nz) - 1, group]
                        if p == cross_end:
                            for case, first in ((at_end(src_z), cross_end), (whole_row, cross_inner)):
                                if step == 1 and case is not whole_row:
                                    continue

                                @pl.when(case)
                                def _():
                                    await_got(sem, wall.at[pl.ds(0, pieces - SINGLES - first)])

                        elif group:

                            @pl.when(jnp.logical_not(rides(step, p, src_z)))
                            def _():
                                await_got(sem, wall.at[p])

                        finish(src_z * nx + xpeer(k), p)

    if nz > 1:
        sent(nz - 1)


def put_kernel(*refs):
    count = (len(refs) - 1) // 2
    sem = refs[-1]
    copies = [pltpu.make_async_copy(refs[i], refs[count + i], sem.at[i]) for i in range(count)]
    for copy in copies:
        copy.start()
    for copy in copies:
        copy.wait()


def per_device(nz, nx, nt, xin, gcot, fcot, scot, lam, proj, gw, gm, gs, vw, vm, vs):
    nfs = nz * nx
    rows, cg = gw.shape
    cv = vw.shape[1]
    cols = cg + cv
    depth, rank = proj.shape
    share = rank // nfs
    pieces = min(PIECES, rows // PIECE_ROWS)
    part = rows // pieces
    dma = pltpu.SemaphoreType.DMA
    shape = jax.ShapeDtypeStruct
    vmem = lambda a: pltpu.VMEM(a.shape, a.dtype)
    results = [
        shape((rows, cg), f32),
        shape((rows, cg), f32),
        shape((depth, cg), bf16),
        shape(gm.shape, f32),
        shape(gs.shape, f32),
        shape((rows, cv), f32),
        shape((rows, cv), f32),
        shape((depth, cv), bf16),
        shape(vm.shape, f32),
        shape(vs.shape, f32),
    ]
    arrays = [xin, gcot, fcot, scot, lam, proj, gw, gm, gs, vw, vm, vs]
    alone = cv == VDIM
    arrays = [
        a if alone and a is lam else pltpu.with_memory_space_constraint(a, pltpu.HBM)
        for a in arrays
    ]
    anywhere = pl.BlockSpec(memory_space=pl.ANY)
    inside = pl.BlockSpec(memory_space=pltpu.VMEM)
    held = pl.pallas_call(
        functools.partial(kernel, nz, nx, nt),
        out_shape=[vmem(a) for a in results],
        in_specs=[
            pl.BlockSpec(memory_space=pltpu.SMEM) if alone and a is lam else anywhere
            for a in (xin, gcot, fcot, scot, lam, proj, gw, gm, gs, vw, vm, vs)
        ],
        out_specs=[inside] * 10,
        scratch_shapes=[
            pltpu.SMEM(lam.shape, lam.dtype),
            vmem(xin),
            vmem(gcot),
            vmem(fcot),
            vmem(scot),
            vmem(proj),
            vmem(gw),
            vmem(vw),
            vmem(gm),
            vmem(gs),
            vmem(vm),
            vmem(vs),
            pltpu.VMEM((nfs * pieces, part, cols), bf16),
            pltpu.VMEM((rank, depth), bf16),
            pltpu.VMEM((rank, rank), bf16),
            pltpu.VMEM((rank, rank), bf16),
            pltpu.VMEM((rank, cols), f32),
            pltpu.VMEM((depth, cols), f32),
            pltpu.VMEM((nx, nz, share, cols), bf16),
            pltpu.VMEM((nx - 1, nz, share, cols), bf16),
            pltpu.VMEM((nz, share, cols), bf16),
            pltpu.VMEM((nz - 2, share, cols), bf16),
            pltpu.VMEM((nz, nx, share, cols), bf16),
            pltpu.VMEM((share, cols), f32),
            pltpu.VMEM((nfs, share, cols), bf16),
            pltpu.VMEM((rank, cols), f32),
            pltpu.VMEM((nt, 2, 8, 128), f32),
            dma((8,)),
            dma((4, DEPTH)),
            dma((2, nz)),
            dma((nz - 1, pieces + 1)),
            dma((nz - 1, (nx - 1) * max(pieces * CROSS_INNER // PIECES, 1))),
            dma((nx - 1, nz)),
            dma((nx - 1, nz - 1, SINGLES + 1)),
            dma((nx - 1, pieces)),
            dma((nx - 1,)),
            dma((nx - 1, nz)),
            dma((1,)),
            dma((1,)),
            dma((1,)),
            dma((nz,)),
            dma((nx - 1,)),
            dma((nx - 1,)),
            dma((1,)),
            dma((1,)),
            pltpu.SemaphoreType.REGULAR((nz - 2,)),
            dma((1,)),
            dma((nz,)),
        ],
        compiler_params=pltpu.CompilerParams(
            collective_id=0, has_side_effects=True, vmem_limit_bytes=40 * 1024 * 1024
        ),
    )(*arrays)
    return tuple(
        pl.pallas_call(
            put_kernel,
            out_shape=results,
            in_specs=[inside] * 10,
            out_specs=[anywhere] * 10,
            scratch_shapes=[dma((10,))],
            compiler_params=pltpu.CompilerParams(vmem_limit_bytes=8 * 1024 * 1024),
        )(*held)
    )


def solution(mesh):
    nz, nx = factor_fs(mesh.shape["fs"])
    assert nz > 3 and nx > 1
    split, whole = P("fs", "tp"), P(None, "tp")
    placed = (P("fs", None), split, split, split, P("tp"), P()) + (split,) * 6
    return jax.shard_map(
        functools.partial(per_device, nz, nx, mesh.shape["tp"]),
        mesh=mesh,
        in_specs=placed,
        out_specs=(split, split, whole, split, split, split, split, whole, split, split),
        check_vma=False,
    )
```

```python
import functools

import jax
import jax.numpy as jnp
from jax import lax
from jax.experimental import pallas as pl
from jax.experimental.pallas import tpu as pltpu
from jax.sharding import PartitionSpec as P

VDIM = 128
PIECES = 8
PIECE_ROWS = 16
CROSS_END = 1
CROSS_INNER = 1
CHUNKS = 4
DEPTH = 3
SINGLES = 2
HOLD_X = 5
HOLD_Z = 5
FIRST_A = (0, 5, 0, 4)
FIRST_B = (5, 8, 4, 7)
FIRST_C = (8, 8, 7, 8)
SECOND = (0, 3, 0, 0)
SECOND_A = (3, 7, 0, 3)
SECOND_B = (7, 8, 3, 8)
THIRD_A = (0, 3, 0, 3)
THIRD_B = (3, 6, 3, 6)
THIRD_C = (6, 8, 6, 8)

moment_decay = 0.9
square_decay = 0.95
adam_floor = 1e-08
learn_rate = 0.02
rms_floor = 0.1

MESH = pl.DeviceIdType.MESH
f32, bf16 = jnp.float32, jnp.bfloat16


def factor_fs(count):
    inner = 1
    while (2 * inner) ** 2 <= count and count % (2 * inner) == 0:
        inner *= 2
    return count // inner, inner


def kernel(
    nz,
    nx,
    nt,
    x_hbm,
    gcot_hbm,
    fcot_hbm,
    scot_hbm,
    lam_hbm,
    proj_hbm,
    gw_hbm,
    gm_hbm,
    gs_hbm,
    vw_hbm,
    vm_hbm,
    vs_hbm,
    new_gw,
    gsteps,
    gcopy,
    new_gm,
    new_gs,
    new_vw,
    vsteps,
    vcopy,
    new_vm,
    new_vs,
    lam_ref,
    xv,
    gcv,
    fcv,
    scv,
    pv,
    gw,
    vw,
    gm,
    gs,
    vm,
    vs,
    wall,
    proj_t,
    gram_high,
    gram_low,
    acc,
    updates,
    rsrc,
    rsx,
    zsrc,
    rsz,
    handed,
    low,
    dall,
    dcat,
    sums,
    in_sem,
    x_sem,
    wz_send,
    wz_recv,
    wz_more,
    wx_send,
    wx_recv,
    wx_own,
    rx_send,
    rx_recv,
    rz_send,
    rz_recv,
    dz_send,
    dz_recv,
    dx_send,
    dx_recv,
    t_send,
    t_recv,
    far_sem,
    hand_send,
    hand_recv,
):
    nfs = nz * nx
    f = lax.axis_index("fs")
    t = lax.axis_index("tp")
    z = lax.div(f, nx)
    x = lax.rem(f, nx)
    rows, cg = gw.shape
    cv = vw.shape[1]
    cols = cg + cv
    rank = acc.shape[0]
    share = rank // nfs
    part = wall.shape[1]
    pieces = rows // part
    tokens = x_hbm.shape[0] // CHUNKS
    cross_end = pieces * CROSS_END // PIECES
    cross_inner = pieces * CROSS_INNER // PIECES
    items = [(k, p) for k in range(nx) for p in range(pieces)]

    def zpeer(k):
        return lax.rem(z + k, nz)

    def xpeer(k):
        return lax.rem(x + k, nx)

    def valid(row):
        return jnp.logical_and(row >= 0, row < nz)

    barrier = pltpu.get_barrier_semaphore()
    for way in (1, -1):

        @pl.when(valid(z + way))
        def _():
            pl.semaphore_signal(barrier, inc=1, device_id=((z + way) * nx + x, t), device_id_type=MESH)

    for k in range(1, nx):
        pl.semaphore_signal(barrier, inc=1, device_id=(z * nx + xpeer(k), t), device_id_type=MESH)
    for k in range(1, nt):
        pl.semaphore_signal(barrier, inc=1, device_id=(f, lax.rem(t + k, nt)), device_id_type=MESH)

    small = [
        pltpu.make_async_copy(src, dst, in_sem.at[(0, 1, 2, 0, 1, 2, 3, 3)[i]])
        for i, (src, dst) in enumerate(
            [
                (gw_hbm, gw),
                (vw_hbm, vw),
                (proj_hbm, pv),
                (gm_hbm, gm),
                (gs_hbm, gs),
                (vm_hbm, vm),
                (vs_hbm, vs),
                (lam_hbm, lam_ref),
            ]
        )
        if src is not lam_hbm or cv > VDIM
    ]
    if cv == VDIM:
        lam_ref = lam_hbm

    def chunk_copies(c):
        at = pl.ds(c * tokens, tokens)
        return [
            pltpu.make_async_copy(src.at[at], dst.at[at], x_sem.at[c % DEPTH])
            for src, dst in [(x_hbm, xv), (gcot_hbm, gcv), (fcot_hbm, fcv), (scot_hbm, scv)]
        ]

    def await_chunk(c):
        wide = tokens * (x_hbm.shape[1] + cg + 2 * cv)
        assert wide % x_hbm.shape[1] == 0
        at = pl.ds(0, wide // x_hbm.shape[1])
        pltpu.make_async_copy(x_hbm.at[at], xv.at[at], x_sem.at[c % DEPTH]).wait()

    for copy in small[:3] + small[7:] + chunk_copies(0):
        copy.start()
    small[0].wait()
    small[1].wait()
    for c in range(1, DEPTH):
        for copy in chunk_copies(c):
            copy.start()
    for p in range(pieces):
        at = pl.ds(p * part, part)
        wall[f * pieces + p, :, :cg] = gw[at, :].astype(bf16)
        wall[f * pieces + p, :, cg:] = vw[at, :].astype(bf16)

    def at_end(row):
        return jnp.logical_or(row == 0, row == nz - 1)

    def crosses(p, row):
        return jnp.logical_or(p < cross_end, jnp.logical_and(p < cross_inner, jnp.logical_not(at_end(row))))

    def wz(way, src_z, k, p, peer, here=False):
        at = (src_z * nx + xpeer(k)) * pieces + p
        away = lax.rem(src_z - (z if here else peer) + nz, nz) - 1
        if k and p >= cross_inner:
            sem = wz_recv.at[away, pieces]
        elif k:
            sem = wz_more.at[away, (k - 1) * max(cross_inner, 1) + p]
        else:
            sem = wz_recv.at[away, p]
        return pltpu.make_async_remote_copy(
            src_ref=wall.at[at],
            dst_ref=wall.at[at],
            send_sem=wz_send.at[(way + 1) // 2, src_z],
            recv_sem=sem,
            device_id=(peer * nx + x, t),
            device_id_type=MESH,
        )

    def wx(k, p, src_z, src_x, own):
        at = (src_z * nx + src_x) * pieces + p
        if own:
            sem = wx_own.at[nx - k - 1, int(p >= HOLD_X)]
        else:
            sem = wx_recv.at[nx - k - 1, lax.rem(src_z - z + nz, nz) - 1, group_of(p)]
        return pltpu.make_async_remote_copy(
            src_ref=wall.at[at],
            dst_ref=wall.at[at],
            send_sem=wx_send.at[k - 1, src_z],
            recv_sem=sem,
            device_id=(z * nx + xpeer(k), t),
            device_id_type=MESH,
        )

    def group_of(p):
        return max(p - (pieces - SINGLES) + 1, 0)

    def await_sent(sem, count):
        pieces_of = wall.at[pl.ds(0, count)]
        pltpu.make_async_remote_copy(
            src_ref=pieces_of,
            dst_ref=pieces_of,
            send_sem=sem,
            recv_sem=sem,
            device_id=(z * nx + xpeer(1), t),
            device_id_type=MESH,
        ).wait_send()

    def await_got(sem, ref):
        pltpu.make_async_remote_copy(
            src_ref=ref,
            dst_ref=ref,
            send_sem=sem,
            recv_sem=sem,
            device_id=(z * nx + xpeer(1), t),
            device_id_type=MESH,
        ).wait_recv()

    def along(src_z, k, p):
        for way in (1, -1):

            @pl.when(valid(z + way))
            def _():
                wz(way, src_z, k, p, z + way).start()

    def over(src_z, p, own=False):
        for k in range(1, nx):
            wx(k, p, src_z, x, own).start()

    def rides(step, p, src_z):
        here = crosses(p, src_z)
        return jnp.logical_or(here, at_end(src_z)) if step < 2 else here

    def relay(step, k, p, where):
        for way in (1, -1):
            src_z = z - way * step
            come = jnp.logical_and(valid(src_z), where)
            if k:
                come = jnp.logical_and(come, crosses(p, src_z))

            @pl.when(come)
            def _():
                wz(way, src_z, k, p, z - way, True).wait_recv()

                @pl.when(valid(z + way))
                def _():
                    wz(way, src_z, k, p, z + way).start()

                if not k:

                    @pl.when(jnp.logical_not(rides(step, p, src_z)))
                    def _():
                        over(src_z, p)

    def relays(step, lo_end, hi_end, lo, hi):
        if step < nz:
            for p in range(pieces):
                ends, rest = lo_end <= p < hi_end, lo <= p < hi
                if ends or rest:
                    where = True if ends and rest else end if ends else jnp.logical_not(end)
                    relay(step, 0, p, where)

    def relay_others(step, where):
        if step < nz:
            for p in range(cross_inner):
                for k in range(1, nx):
                    relay(step, k, p, where)

    def turns(lo, hi):
        lo, hi = min(lo, pieces), min(hi, pieces)
        for k in range(1, nx):
            if lo < hi:
                await_got(wx_own.at[k - 1, int(lo >= HOLD_X)], wall.at[pl.ds(lo, hi - lo)])
            for p in range(lo, hi):

                @pl.when(rides(0, p, z))
                def _():
                    along(z, k, p)

    def sent(step):
        for way in (1, -1) if step else (0,):
            src_z = z - way * step
            src_end = at_end(src_z)
            for case, many, crossing, passed in (
                (src_end, cross_end if step else pieces, cross_end, step == 1),
                (jnp.logical_not(src_end), cross_inner, cross_inner, False),
            ):

                @pl.when(jnp.logical_and(valid(src_z), case))
                def _():
                    for go in (way,) if step else (1, -1):

                        @pl.when(valid(z + go))
                        def _():
                            await_sent(wz_send.at[(go + 1) // 2, src_z], pieces + (nx - 1) * many)

                    if not passed:
                        for k in range(1, nx):
                            await_sent(wx_send.at[k - 1, src_z], pieces - crossing if step else pieces)

    end = at_end(z)
    next_rows = jnp.where(valid(z + 1), 1, 0) + jnp.where(valid(z - 1), 1, 0)

    def tell(i):
        if i < nz - 2:
            for way in (1, -1):

                @pl.when(valid(z + way))
                def _():
                    pl.semaphore_signal(
                        far_sem.at[i], inc=1, device_id=((z + way) * nx + x, t), device_id_type=MESH
                    )

    def hear(i):
        if i < nz - 2:
            pl.semaphore_wait(far_sem.at[i], next_rows)

    pl.semaphore_wait(barrier, next_rows + (nx - 1) + (nt - 1))
    tell(0)
    for p in range(pieces):
        if p < HOLD_Z:
            along(z, 0, p)
        else:

            @pl.when(jnp.logical_not(end))
            def _():
                along(z, 0, p)

        if p < HOLD_X:
            over(z, p, True)

    for copy in small[2:3] + small[7:]:
        copy.wait()
    proj_t[...] = pv[...].T
    head = lax.broadcasted_iota(jnp.int32, (1, cv), 1) // VDIM
    lam = jnp.zeros((1, cv), f32)
    for h in range(cv // VDIM):
        lam = jnp.where(head == h, lam_ref[h], lam)
    for c in range(CHUNKS):
        await_chunk(c)
        if c + DEPTH < CHUNKS:
            for copy in chunk_copies(c + DEPTH):
                copy.start()
        elif c + DEPTH == CHUNKS:
            for i in range(3, 7):
                small[i].start()
        at = pl.ds(c * tokens, tokens)
        upper = lax.dot_general(
            proj_t[...], xv[at, :], (((1,), (1,)), ((), ())), preferred_element_type=f32
        ).astype(bf16)
        value = (fcv[at, :].astype(f32) - lam * scv[at, :].astype(f32)).astype(bf16)
        gate_part = jnp.dot(upper, gcv[at, :], preferred_element_type=f32)
        value_part = jnp.dot(upper, value, preferred_element_type=f32)
        if c:
            gate_part += acc[:, :cg]
            value_part += acc[:, cg:]
        acc[:, :cg] = gate_part
        acc[:, cg:] = value_part
        if c % 2:
            hear(c // 2)
            tell(c // 2 + 1)

    for i in range(CHUNKS // 2, nz - 2):
        hear(i)
        tell(i + 1)
    for zi in range(nz):
        for xi in range(nx):
            at = pl.ds((zi * nx + xi) * share, share)
            rsrc[xi, zi] = acc[at, :].astype(bf16)

    def rx(k, zi):
        return pltpu.make_async_remote_copy(
            src_ref=rsrc.at[xpeer(k), zi],
            dst_ref=rsx.at[nx - k - 1, zi],
            send_sem=rx_send.at[k - 1],
            recv_sem=rx_recv.at[nx - k - 1, zi],
            device_id=(z * nx + xpeer(k), t),
            device_id_type=MESH,
        )

    def hand(k, zi):
        row = jnp.where(z == 0, 1, nz - 2)
        return pltpu.make_async_remote_copy(
            src_ref=rsrc.at[xpeer(k), zi],
            dst_ref=handed.at[zi, (nx - k) % nx],
            send_sem=hand_send.at[0],
            recv_sem=hand_recv.at[zi],
            device_id=(row * nx + xpeer(k), t),
            device_id_type=MESH,
        )

    def rz(zi):
        return pltpu.make_async_remote_copy(
            src_ref=zsrc.at[zi],
            dst_ref=rsz.at[z - 1],
            send_sem=rz_send.at[0],
            recv_sem=rz_recv.at[0],
            device_id=(zi * nx + x, t),
            device_id_type=MESH,
        )

    far = list(range(1, nz))

    def other(j):
        return jnp.where(2 * z < nz, lax.rem(z + nz - j, nz), zpeer(j))

    def handing(j):
        return jnp.where(z == 0, nz - j, j - 1)

    inner = jnp.logical_not(end)
    beside = jnp.logical_or(z == 1, z == nz - 2)

    def row_sum(zi):
        at = pl.ds(pl.multiple_of((zi * nx + x) * share, share), share)
        low[...] = acc[at, :]
        for k in range(1, nx):
            await_got(rx_recv.at[k - 1, zi], rsx.at[0, 0])
            low[...] += rsx[k - 1, zi].astype(f32)

        @pl.when(jnp.logical_and(beside, zi != jnp.where(z == 1, 0, nz - 1)))
        def _():
            await_got(hand_recv.at[zi], handed.at[0])
            for k in range(nx):
                low[...] += handed[zi, k].astype(f32)

    @pl.when(inner)
    def _():
        for j in far:
            for k in range(1, nx):
                rx(k, other(j)).start()

    @pl.when(end)
    def _():
        for j in far:
            for k in list(range(1, nx)) + [0]:
                hand(k, handing(j)).start()

    for k in range(1, nx):
        rx(k, z).start()

    def rest_over():
        for p in range(min(HOLD_X, pieces), pieces):
            over(z, p, True)

    pl.when(end)(rest_over)

    @pl.when(end)
    def _():
        for p in range(min(HOLD_Z, pieces), pieces):
            along(z, 0, p)

    relays(1, *FIRST_A)
    gram = jnp.dot(proj_t[...], pv[...], preferred_element_type=f32)
    gram_high[...] = gram.astype(bf16)
    gram_low[...] = (gram - gram_high[...].astype(f32)).astype(bf16)

    @pl.when(inner)
    def _():
        for j in far:
            row_sum(other(j))
            zsrc[other(j)] = low[...].astype(bf16)
            rz(other(j)).start()

    pl.when(inner)(rest_over)
    relays(1, *FIRST_B)
    relays(2, *SECOND)
    for i in range(3, 7):
        small[i].wait()
    row_sum(z)

    @pl.when(end)
    def _():
        await_got(rz_recv.at[0], rsz.at[pl.ds(0, nz - 2)])

    @pl.when(inner)
    def _():
        await_got(rz_recv.at[0], rsz.at[pl.ds(0, nz - 3)])

    for row in range(1, nz - 1):

        @pl.when(z != row)
        def _():
            low[...] += rsz[row - 1].astype(f32)

    for first, second, new_m, new_s, at in (
        (gm, gs, new_gm, new_gs, slice(0, cg)),
        (vm, vs, new_vm, new_vs, slice(cg, cols)),
    ):
        mine = low[:, at]
        new_first = moment_decay * first[...] + (1.0 - moment_decay) * mine
        new_second = square_decay * second[...] + (1.0 - square_decay) * mine * mine
        new_m[...] = new_first
        new_s[...] = new_second
        dall[f, :, at] = (new_first / (jnp.sqrt(new_second) + adam_floor)).astype(bf16)

    def dz(k, src_z):
        owner = src_z * nx + x
        return pltpu.make_async_remote_copy(
            src_ref=dall.at[owner],
            dst_ref=dall.at[owner],
            send_sem=dz_send.at[0],
            recv_sem=dz_recv.at[src_z],
            device_id=(zpeer(k) * nx + x, t),
            device_id_type=MESH,
        )

    def dx(k, src_z, src_x):
        owner = src_z * nx + src_x
        return pltpu.make_async_remote_copy(
            src_ref=dall.at[owner],
            dst_ref=dall.at[owner],
            send_sem=dx_send.at[k - 1],
            recv_sem=dx_recv.at[nx - k - 1],
            device_id=(z * nx + xpeer(k), t),
            device_id_type=MESH,
        )

    for k in range(1, nz):
        dz(k, z).start()
    for m in range(1, nx):
        dx(m, z, x).start()
    relays(1, *FIRST_C)
    turns(0, HOLD_X)
    relays(2, *SECOND_A)
    for k in range(1, nz):
        dz(k, zpeer(k)).wait_recv()
        for m in range(1, nx):
            dx(m, zpeer(k), x).start()
    relays(2, *SECOND_B)
    turns(HOLD_X, pieces)
    relay_others(1, inner)
    relays(3, *THIRD_A)
    for step in range(2, nz):
        relay_others(step, inner)
    for m in range(1, nx):
        await_got(dx_recv.at[m - 1], dall.at[pl.ds(0, nz)])

    for j in range(nfs):
        dcat[pl.ds(j * share, share), :] = dall[j].astype(f32)
    direction = dcat[...].astype(bf16)

    turned = jnp.dot(gram_high[...], direction, preferred_element_type=f32)
    turned += jnp.dot(gram_low[...], direction, preferred_element_type=f32)
    squares = jnp.sum((turned * dcat[...]).reshape(rank // 8, 8, cols), axis=0)
    squares = jnp.sum(squares, axis=0, keepdims=True)
    squares = jnp.maximum(squares, 0.0)
    gate_sum = jnp.sum(squares[:, :cg], axis=1, keepdims=True)
    value_sum = jnp.sum(squares[:, cg:], axis=1, keepdims=True)
    sums[t, 0] = jnp.broadcast_to(gate_sum, (8, 128))
    sums[t, 1] = jnp.broadcast_to(value_sum, (8, 128))

    def tp(k, src_t):
        return pltpu.make_async_remote_copy(
            src_ref=sums.at[src_t],
            dst_ref=sums.at[src_t],
            send_sem=t_send.at[0],
            recv_sem=t_recv.at[0],
            device_id=(f, lax.rem(t + k, nt)),
            device_id_type=MESH,
        )

    for k in range(1, nt):
        tp(k, t).start()

    def expand(j, carry):
        at = pl.ds(pl.multiple_of(j * rows, rows), rows)
        updates[at, :] = jnp.dot(pv[at, :], direction, preferred_element_type=f32)
        return carry

    lax.fori_loop(0, nfs // 2, expand, 0, unroll=2)
    relays(3, *THIRD_B)
    lax.fori_loop(nfs // 2, nfs, expand, 0, unroll=2)
    relays(3, *THIRD_C)
    for step in range(4, nz):
        relays(step, 0, pieces, 0, pieces)
    for way in (1, -1):

        @pl.when(jnp.logical_and(valid(z - way), at_end(z - way)))
        def _():
            for p in range(cross_end, cross_inner):
                for k in range(1, nx):
                    wz(way, z - way, k, p, z - way, True).wait_recv()
            await_got(wz_recv.at[lax.rem(nz - way, nz) - 1, pieces], wall.at[pl.ds(0, (nx - 1) * (pieces - cross_inner))])

    await_got(t_recv.at[0], sums.at[pl.ds(0, nt - 1)])
    whole = sums[0]
    for k in range(1, nt):
        whole = whole + sums[k]
    entries = nfs * rows * nt
    gscale = (1.0 / (jnp.sqrt(whole[0] / (entries * cg)) + rms_floor))[0:1, 0:1]
    vscale = (1.0 / (jnp.sqrt(whole[1] / (entries * cv)) + rms_floor))[0:1, 0:1]

    at = pl.ds(pl.multiple_of(f * rows, rows), rows)
    gstep = updates[at, :cg] * gscale
    vstep = updates[at, cg:] * vscale
    gsteps[...] = gstep
    vsteps[...] = vstep
    new_gw[...] = gw[...] - learn_rate * gstep
    new_vw[...] = vw[...] - learn_rate * vstep

    def finish(j, p):
        at = pl.ds(pl.multiple_of(j * rows + p * part, part), part)
        held = wall[j * pieces + p].astype(f32)
        update = updates[at, :]
        gcopy[at, :] = (held[:, :cg] - learn_rate * (update[:, :cg] * gscale)).astype(bf16)
        vcopy[at, :] = (held[:, cg:] - learn_rate * (update[:, cg:] * vscale)).astype(bf16)

    def finish_block(j, lo, hi):
        def body(p, carry):
            finish(j, p)
            return carry

        lax.fori_loop(lo, hi, body, 0, unroll=True)

    for zi in range(nz):
        finish_block(zi * nx + x, 0, pieces)
    for k in range(1, nx):
        finish_block(z * nx + xpeer(k), 0, pieces)

    @pl.when(inner)
    def _():
        await_got(rz_send.at[0], zsrc.at[pl.ds(0, nz - 1)])
        for m in range(1, nx):
            await_got(rx_send.at[m - 1], rsrc.at[0])

    @pl.when(end)
    def _():
        await_got(hand_send.at[0], handed.at[pl.ds(0, nz - 1)])
        for m in range(1, nx):
            await_got(rx_send.at[m - 1], rsrc.at[0, 0])

    await_got(dz_send.at[0], dall.at[pl.ds(0, nz - 1)])
    for m in range(1, nx):
        await_got(dx_send.at[m - 1], dall.at[pl.ds(0, nz)])
    await_got(t_send.at[0], sums.at[pl.ds(0, nt - 1)])
    for step in range(max(nz - 1, 1)):
        sent(step)
    for step in range(1, nz):
        relay_others(step, end)
    if cross_end:
        for zi in range(1, nz):
            for k in range(1, nx):
                finish_block(zpeer(zi) * nx + xpeer(k), 0, cross_end)
    for step in range(1, nz):
        for p in range(cross_end, pieces):
            for way in (1, -1):
                src_z = z - way * step

                @pl.when(valid(src_z))
                def _():
                    for k in range(1, nx):
                        group = group_of(p)
                        whole_row = jnp.logical_not(at_end(src_z))
                        sem = wx_recv.at[k - 1, lax.rem(src_z - z + nz, nz) - 1, group]
                        if p == cross_end:
                            for case, first in ((at_end(src_z), cross_end), (whole_row, cross_inner)):
                                if step == 1 and case is not whole_row:
                                    continue

                                @pl.when(case)
                                def _():
                                    await_got(sem, wall.at[pl.ds(0, pieces - SINGLES - first)])

                        elif group:

                            @pl.when(jnp.logical_not(rides(step, p, src_z)))
                            def _():
                                await_got(sem, wall.at[p])

                        finish(src_z * nx + xpeer(k), p)

    if nz > 1:
        sent(nz - 1)


def put_kernel(*refs):
    count = (len(refs) - 1) // 2
    sem = refs[-1]
    copies = [pltpu.make_async_copy(refs[i], refs[count + i], sem.at[i]) for i in range(count)]
    for copy in copies:
        copy.start()
    for copy in copies:
        copy.wait()


def per_device(nz, nx, nt, xin, gcot, fcot, scot, lam, proj, gw, gm, gs, vw, vm, vs):
    nfs = nz * nx
    rows, cg = gw.shape
    cv = vw.shape[1]
    cols = cg + cv
    depth, rank = proj.shape
    share = rank // nfs
    pieces = min(PIECES, rows // PIECE_ROWS)
    part = rows // pieces
    dma = pltpu.SemaphoreType.DMA
    shape = jax.ShapeDtypeStruct
    vmem = lambda a: pltpu.VMEM(a.shape, a.dtype)
    results = [
        shape((rows, cg), f32),
        shape((rows, cg), f32),
        shape((depth, cg), bf16),
        shape(gm.shape, f32),
        shape(gs.shape, f32),
        shape((rows, cv), f32),
        shape((rows, cv), f32),
        shape((depth, cv), bf16),
        shape(vm.shape, f32),
        shape(vs.shape, f32),
    ]
    arrays = [xin, gcot, fcot, scot, lam, proj, gw, gm, gs, vw, vm, vs]
    alone = cv == VDIM
    arrays = [
        a if alone and a is lam else pltpu.with_memory_space_constraint(a, pltpu.HBM)
        for a in arrays
    ]
    anywhere = pl.BlockSpec(memory_space=pl.ANY)
    inside = pl.BlockSpec(memory_space=pltpu.VMEM)
    held = pl.pallas_call(
        functools.partial(kernel, nz, nx, nt),
        out_shape=[vmem(a) for a in results],
        in_specs=[
            pl.BlockSpec(memory_space=pltpu.SMEM) if alone and a is lam else anywhere
            for a in (xin, gcot, fcot, scot, lam, proj, gw, gm, gs, vw, vm, vs)
        ],
        out_specs=[inside] * 10,
        scratch_shapes=[
            pltpu.SMEM(lam.shape, lam.dtype),
            vmem(xin),
            vmem(gcot),
            vmem(fcot),
            vmem(scot),
            vmem(proj),
            vmem(gw),
            vmem(vw),
            vmem(gm),
            vmem(gs),
            vmem(vm),
            vmem(vs),
            pltpu.VMEM((nfs * pieces, part, cols), bf16),
            pltpu.VMEM((rank, depth), bf16),
            pltpu.VMEM((rank, rank), bf16),
            pltpu.VMEM((rank, rank), bf16),
            pltpu.VMEM((rank, cols), f32),
            pltpu.VMEM((depth, cols), f32),
            pltpu.VMEM((nx, nz, share, cols), bf16),
            pltpu.VMEM((nx - 1, nz, share, cols), bf16),
            pltpu.VMEM((nz, share, cols), bf16),
            pltpu.VMEM((nz - 2, share, cols), bf16),
            pltpu.VMEM((nz, nx, share, cols), bf16),
            pltpu.VMEM((share, cols), f32),
            pltpu.VMEM((nfs, share, cols), bf16),
            pltpu.VMEM((rank, cols), f32),
            pltpu.VMEM((nt, 2, 8, 128), f32),
            dma((4,)),
            dma((DEPTH,)),
            dma((2, nz)),
            dma((nz - 1, pieces + 1)),
            dma((nz - 1, (nx - 1) * max(pieces * CROSS_INNER // PIECES, 1))),
            dma((nx - 1, nz)),
            dma((nx - 1, nz - 1, SINGLES + 1)),
            dma((nx - 1, 2)),
            dma((nx - 1,)),
            dma((nx - 1, nz)),
            dma((1,)),
            dma((1,)),
            dma((1,)),
            dma((nz,)),
            dma((nx - 1,)),
            dma((nx - 1,)),
            dma((1,)),
            dma((1,)),
            pltpu.SemaphoreType.REGULAR((nz - 2,)),
            dma((1,)),
            dma((nz,)),
        ],
        compiler_params=pltpu.CompilerParams(
            collective_id=0, has_side_effects=True, vmem_limit_bytes=40 * 1024 * 1024
        ),
    )(*arrays)
    return tuple(
        pl.pallas_call(
            put_kernel,
            out_shape=results,
            in_specs=[inside] * 10,
            out_specs=[anywhere] * 10,
            scratch_shapes=[dma((10,))],
            compiler_params=pltpu.CompilerParams(vmem_limit_bytes=8 * 1024 * 1024),
        )(*held)
    )


def solution(mesh):
    nz, nx = factor_fs(mesh.shape["fs"])
    assert nz > 3 and nx > 1
    split, whole = P("fs", "tp"), P(None, "tp")
    placed = (P("fs", None), split, split, split, P("tp"), P()) + (split,) * 6
    return jax.shard_map(
        functools.partial(per_device, nz, nx, mesh.shape["tp"]),
        mesh=mesh,
        in_specs=placed,
        out_specs=(split, split, whole, split, split, split, split, whole, split, split),
        check_vma=False,
    )
```

```python
import functools

import jax
import jax.numpy as jnp
from jax import lax
from jax.experimental import pallas as pl
from jax.experimental.pallas import tpu as pltpu
from jax.sharding import PartitionSpec as P

VDIM = 128
PIECES = 8
PIECE_ROWS = 16
CROSS_END = 2
CROSS_INNER = 1
CHUNKS = 4
DEPTH = 3
SINGLES = 2
HOLD_X = 5
HOLD_Z = 5
FIRST_A = (0, 5, 0, 4)
FIRST_B = (5, 8, 4, 7)
FIRST_C = (8, 8, 7, 8)
SECOND = (0, 4, 0, 0)
SECOND_A = (4, 7, 0, 3)
SECOND_B = (7, 8, 3, 8)
THIRD_A = (0, 3, 0, 3)
THIRD_B = (3, 6, 3, 6)
THIRD_C = (6, 8, 6, 8)

moment_decay = 0.9
square_decay = 0.95
adam_floor = 1e-08
learn_rate = 0.02
rms_floor = 0.1

MESH = pl.DeviceIdType.MESH
f32, bf16 = jnp.float32, jnp.bfloat16


def factor_fs(count):
    inner = 1
    while (2 * inner) ** 2 <= count and count % (2 * inner) == 0:
        inner *= 2
    return count // inner, inner


def kernel(
    nz,
    nx,
    nt,
    x_hbm,
    gcot_hbm,
    fcot_hbm,
    scot_hbm,
    lam_hbm,
    proj_hbm,
    gw_hbm,
    gm_hbm,
    gs_hbm,
    vw_hbm,
    vm_hbm,
    vs_hbm,
    new_gw,
    gsteps,
    gcopy,
    new_gm,
    new_gs,
    new_vw,
    vsteps,
    vcopy,
    new_vm,
    new_vs,
    lam_ref,
    xv,
    gcv,
    fcv,
    scv,
    pv,
    gw,
    vw,
    gm,
    gs,
    vm,
    vs,
    wall,
    proj_t,
    gram_high,
    gram_low,
    acc,
    updates,
    rsrc,
    rsx,
    zsrc,
    rsz,
    handed,
    low,
    dall,
    dcat,
    sums,
    in_sem,
    x_sem,
    wz_send,
    wz_recv,
    wz_more,
    wx_send,
    wx_recv,
    wx_own,
    rx_send,
    rx_recv,
    rz_send,
    rz_recv,
    dz_send,
    dz_recv,
    dx_send,
    dx_recv,
    t_send,
    t_recv,
    far_sem,
    hand_send,
    hand_recv,
):
    nfs = nz * nx
    f = lax.axis_index("fs")
    t = lax.axis_index("tp")
    z = lax.div(f, nx)
    x = lax.rem(f, nx)
    rows, cg = gw.shape
    cv = vw.shape[1]
    cols = cg + cv
    rank = acc.shape[0]
    share = rank // nfs
    part = wall.shape[1]
    pieces = rows // part
    tokens = x_hbm.shape[0] // CHUNKS
    cross_end = pieces * CROSS_END // PIECES
    cross_inner = pieces * CROSS_INNER // PIECES
    cross_most = max(cross_end, cross_inner)
    cross_least = min(cross_end, cross_inner)
    items = [(k, p) for k in range(nx) for p in range(pieces)]

    def zpeer(k):
        return lax.rem(z + k, nz)

    def xpeer(k):
        return lax.rem(x + k, nx)

    def valid(row):
        return jnp.logical_and(row >= 0, row < nz)

    barrier = pltpu.get_barrier_semaphore()
    for way in (1, -1):

        @pl.when(valid(z + way))
        def _():
            pl.semaphore_signal(barrier, inc=1, device_id=((z + way) * nx + x, t), device_id_type=MESH)

    for k in range(1, nx):
        pl.semaphore_signal(barrier, inc=1, device_id=(z * nx + xpeer(k), t), device_id_type=MESH)
    for k in range(1, nt):
        pl.semaphore_signal(barrier, inc=1, device_id=(f, lax.rem(t + k, nt)), device_id_type=MESH)

    small = [
        pltpu.make_async_copy(src, dst, in_sem.at[(0, 1, 2, 0, 1, 2, 3, 3)[i]])
        for i, (src, dst) in enumerate(
            [
                (gw_hbm, gw),
                (vw_hbm, vw),
                (proj_hbm, pv),
                (gm_hbm, gm),
                (gs_hbm, gs),
                (vm_hbm, vm),
                (vs_hbm, vs),
                (lam_hbm, lam_ref),
            ]
        )
        if src is not lam_hbm or cv > VDIM
    ]
    if cv == VDIM:
        lam_ref = lam_hbm

    def chunk_copies(c):
        at = pl.ds(c * tokens, tokens)
        return [
            pltpu.make_async_copy(src.at[at], dst.at[at], x_sem.at[c % DEPTH])
            for src, dst in [(x_hbm, xv), (gcot_hbm, gcv), (fcot_hbm, fcv), (scot_hbm, scv)]
        ]

    def await_chunk(c):
        wide = tokens * (x_hbm.shape[1] + cg + 2 * cv)
        assert wide % x_hbm.shape[1] == 0
        at = pl.ds(0, wide // x_hbm.shape[1])
        pltpu.make_async_copy(x_hbm.at[at], xv.at[at], x_sem.at[c % DEPTH]).wait()

    for copy in small[:3] + small[7:] + chunk_copies(0):
        copy.start()
    small[0].wait()
    small[1].wait()
    for c in range(1, DEPTH):
        for copy in chunk_copies(c):
            copy.start()
    for p in range(pieces):
        at = pl.ds(p * part, part)
        wall[f * pieces + p, :, :cg] = gw[at, :].astype(bf16)
        wall[f * pieces + p, :, cg:] = vw[at, :].astype(bf16)
    def at_end(row):
        return jnp.logical_or(row == 0, row == nz - 1)

    def crosses(p, row):
        return jnp.where(at_end(row), p < cross_end, p < cross_inner)

    def wz(way, src_z, k, p, peer, here=False):
        at = (src_z * nx + xpeer(k)) * pieces + p
        away = lax.rem(src_z - (z if here else peer) + nz, nz) - 1
        if k and p >= cross_most:
            sem = wz_recv.at[away, pieces]
        elif k:
            sem = wz_more.at[away, (k - 1) * max(cross_most, 1) + p]
        else:
            sem = wz_recv.at[away, p]
        return pltpu.make_async_remote_copy(
            src_ref=wall.at[at],
            dst_ref=wall.at[at],
            send_sem=wz_send.at[(way + 1) // 2, src_z],
            recv_sem=sem,
            device_id=(peer * nx + x, t),
            device_id_type=MESH,
        )

    def wx(k, p, src_z, src_x, own):
        at = (src_z * nx + src_x) * pieces + p
        if own:
            sem = wx_own.at[nx - k - 1, int(p >= HOLD_X)]
        else:
            sem = wx_recv.at[nx - k - 1, lax.rem(src_z - z + nz, nz) - 1, group_of(p)]
        return pltpu.make_async_remote_copy(
            src_ref=wall.at[at],
            dst_ref=wall.at[at],
            send_sem=wx_send.at[k - 1, src_z],
            recv_sem=sem,
            device_id=(z * nx + xpeer(k), t),
            device_id_type=MESH,
        )

    def group_of(p):
        return max(p - (pieces - SINGLES) + 1, 0)

    def await_sent(sem, count):
        pieces_of = wall.at[pl.ds(0, count)]
        pltpu.make_async_remote_copy(
            src_ref=pieces_of,
            dst_ref=pieces_of,
            send_sem=sem,
            recv_sem=sem,
            device_id=(z * nx + xpeer(1), t),
            device_id_type=MESH,
        ).wait_send()

    def await_got(sem, ref):
        pltpu.make_async_remote_copy(
            src_ref=ref,
            dst_ref=ref,
            send_sem=sem,
            recv_sem=sem,
            device_id=(z * nx + xpeer(1), t),
            device_id_type=MESH,
        ).wait_recv()

    def along(src_z, k, p):
        for way in (1, -1):

            @pl.when(valid(z + way))
            def _():
                wz(way, src_z, k, p, z + way).start()

    def over(src_z, p, own=False):
        for k in range(1, nx):
            wx(k, p, src_z, x, own).start()

    def rides(step, p, src_z):
        here = crosses(p, src_z)
        return jnp.logical_or(here, at_end(src_z)) if step < 2 else here

    def relay(step, k, p, where):
        for way in (1, -1):
            src_z = z - way * step
            come = jnp.logical_and(valid(src_z), where)
            if k:
                come = jnp.logical_and(come, crosses(p, src_z))

            @pl.when(come)
            def _():
                wz(way, src_z, k, p, z - way, True).wait_recv()

                @pl.when(valid(z + way))
                def _():
                    wz(way, src_z, k, p, z + way).start()

                if not k:

                    @pl.when(jnp.logical_not(rides(step, p, src_z)))
                    def _():
                        over(src_z, p)

    def relays(step, lo_end, hi_end, lo, hi):
        if step < nz:
            for p in range(pieces):
                ends, rest = lo_end <= p < hi_end, lo <= p < hi
                if ends or rest:
                    where = True if ends and rest else end if ends else jnp.logical_not(end)
                    relay(step, 0, p, where)

    def relay_others(step, where):
        if step < nz:
            for p in range(cross_most):
                for k in range(1, nx):
                    relay(step, k, p, where)

    def turns(lo, hi):
        lo, hi = min(lo, pieces), min(hi, pieces)
        for k in range(1, nx):
            if lo < hi:
                await_got(wx_own.at[k - 1, int(lo >= HOLD_X)], wall.at[pl.ds(lo, hi - lo)])
            for p in range(lo, hi):

                @pl.when(rides(0, p, z))
                def _():
                    along(z, k, p)

    def sent(step):
        for way in (1, -1) if step else (0,):
            src_z = z - way * step
            src_end = at_end(src_z)
            for case, many, crossing, passed in (
                (src_end, cross_end if step else pieces, cross_end, step == 1),
                (jnp.logical_not(src_end), cross_inner, cross_inner, False),
            ):

                @pl.when(jnp.logical_and(valid(src_z), case))
                def _():
                    for go in (way,) if step else (1, -1):

                        @pl.when(valid(z + go))
                        def _():
                            await_sent(wz_send.at[(go + 1) // 2, src_z], pieces + (nx - 1) * many)

                    if not passed:
                        for k in range(1, nx):
                            await_sent(wx_send.at[k - 1, src_z], pieces - crossing if step else pieces)

    end = at_end(z)
    next_rows = jnp.where(valid(z + 1), 1, 0) + jnp.where(valid(z - 1), 1, 0)

    def tell(i):
        if i < nz - 2:
            for way in (1, -1):

                @pl.when(valid(z + way))
                def _():
                    pl.semaphore_signal(
                        far_sem.at[i], inc=1, device_id=((z + way) * nx + x, t), device_id_type=MESH
                    )

    def hear(i):
        if i < nz - 2:
            pl.semaphore_wait(far_sem.at[i], next_rows)

    pl.semaphore_wait(barrier, next_rows + (nx - 1) + (nt - 1))
    tell(0)
    for p in range(pieces):
        if p < HOLD_Z:
            along(z, 0, p)
        else:

            @pl.when(jnp.logical_not(end))
            def _():
                along(z, 0, p)

        if p < HOLD_X:
            over(z, p, True)
    for copy in small[2:3] + small[7:]:
        copy.wait()
    proj_t[...] = pv[...].T
    head = lax.broadcasted_iota(jnp.int32, (1, cv), 1) // VDIM
    lam = jnp.zeros((1, cv), f32)
    for h in range(cv // VDIM):
        lam = jnp.where(head == h, lam_ref[h], lam)
    for c in range(CHUNKS):
        await_chunk(c)
        if c + DEPTH < CHUNKS:
            for copy in chunk_copies(c + DEPTH):
                copy.start()
        elif c + DEPTH == CHUNKS:
            for i in range(3, 7):
                small[i].start()
        at = pl.ds(c * tokens, tokens)
        upper = lax.dot_general(
            proj_t[...], xv[at, :], (((1,), (1,)), ((), ())), preferred_element_type=f32
        ).astype(bf16)
        value = (fcv[at, :].astype(f32) - lam * scv[at, :].astype(f32)).astype(bf16)
        gate_part = jnp.dot(upper, gcv[at, :], preferred_element_type=f32)
        value_part = jnp.dot(upper, value, preferred_element_type=f32)
        if c:
            gate_part += acc[:, :cg]
            value_part += acc[:, cg:]
        acc[:, :cg] = gate_part
        acc[:, cg:] = value_part
        if c % 2:
            hear(c // 2)
            tell(c // 2 + 1)

    for i in range(CHUNKS // 2, nz - 2):
        hear(i)
        tell(i + 1)
    for zi in range(nz):
        for xi in range(nx):
            at = pl.ds((zi * nx + xi) * share, share)
            rsrc[xi, zi] = acc[at, :].astype(bf16)

    def rx(k, zi):
        return pltpu.make_async_remote_copy(
            src_ref=rsrc.at[xpeer(k), zi],
            dst_ref=rsx.at[nx - k - 1, zi],
            send_sem=rx_send.at[k - 1],
            recv_sem=rx_recv.at[nx - k - 1, zi],
            device_id=(z * nx + xpeer(k), t),
            device_id_type=MESH,
        )

    def hand(k, zi):
        row = jnp.where(z == 0, 1, nz - 2)
        return pltpu.make_async_remote_copy(
            src_ref=rsrc.at[xpeer(k), zi],
            dst_ref=handed.at[zi, (nx - k) % nx],
            send_sem=hand_send.at[0],
            recv_sem=hand_recv.at[zi],
            device_id=(row * nx + xpeer(k), t),
            device_id_type=MESH,
        )

    def rz(zi):
        return pltpu.make_async_remote_copy(
            src_ref=zsrc.at[zi],
            dst_ref=rsz.at[z - 1],
            send_sem=rz_send.at[0],
            recv_sem=rz_recv.at[0],
            device_id=(zi * nx + x, t),
            device_id_type=MESH,
        )

    far = list(range(1, nz))

    def other(j):
        return jnp.where(2 * z < nz, lax.rem(z + nz - j, nz), zpeer(j))

    def handing(j):
        return jnp.where(z == 0, nz - j, j - 1)

    inner = jnp.logical_not(end)
    beside = jnp.logical_or(z == 1, z == nz - 2)

    def row_sum(zi):
        at = pl.ds(pl.multiple_of((zi * nx + x) * share, share), share)
        low[...] = acc[at, :]
        for k in range(1, nx):
            await_got(rx_recv.at[k - 1, zi], rsx.at[0, 0])
            low[...] += rsx[k - 1, zi].astype(f32)

        @pl.when(jnp.logical_and(beside, zi != jnp.where(z == 1, 0, nz - 1)))
        def _():
            await_got(hand_recv.at[zi], handed.at[0])
            for k in range(nx):
                low[...] += handed[zi, k].astype(f32)

    @pl.when(inner)
    def _():
        for j in far:
            for k in range(1, nx):
                rx(k, other(j)).start()

    @pl.when(end)
    def _():
        for j in far:
            for k in list(range(1, nx)) + [0]:
                hand(k, handing(j)).start()

    for k in range(1, nx):
        rx(k, z).start()
    def rest_over():
        for p in range(min(HOLD_X, pieces), pieces):
            over(z, p, True)

    pl.when(end)(rest_over)

    @pl.when(end)
    def _():
        for p in range(min(HOLD_Z, pieces), pieces):
            along(z, 0, p)

    relays(1, *FIRST_A)
    gram = jnp.dot(proj_t[...], pv[...], preferred_element_type=f32)
    gram_high[...] = gram.astype(bf16)
    gram_low[...] = (gram - gram_high[...].astype(f32)).astype(bf16)
    @pl.when(inner)
    def _():
        for j in far:
            row_sum(other(j))
            zsrc[other(j)] = low[...].astype(bf16)
            rz(other(j)).start()

    pl.when(inner)(rest_over)
    relays(1, *FIRST_B)
    relays(2, *SECOND)
    for i in range(3, 7):
        small[i].wait()
    row_sum(z)

    @pl.when(end)
    def _():
        await_got(rz_recv.at[0], rsz.at[pl.ds(0, nz - 2)])

    @pl.when(inner)
    def _():
        await_got(rz_recv.at[0], rsz.at[pl.ds(0, nz - 3)])

    for row in range(1, nz - 1):

        @pl.when(z != row)
        def _():
            low[...] += rsz[row - 1].astype(f32)
    for first, second, new_m, new_s, at in (
        (gm, gs, new_gm, new_gs, slice(0, cg)),
        (vm, vs, new_vm, new_vs, slice(cg, cols)),
    ):
        mine = low[:, at]
        new_first = moment_decay * first[...] + (1.0 - moment_decay) * mine
        new_second = square_decay * second[...] + (1.0 - square_decay) * mine * mine
        new_m[...] = new_first
        new_s[...] = new_second
        dall[f, :, at] = (new_first / (jnp.sqrt(new_second) + adam_floor)).astype(bf16)

    def dz(k, src_z):
        owner = src_z * nx + x
        return pltpu.make_async_remote_copy(
            src_ref=dall.at[owner],
            dst_ref=dall.at[owner],
            send_sem=dz_send.at[0],
            recv_sem=dz_recv.at[src_z],
            device_id=(zpeer(k) * nx + x, t),
            device_id_type=MESH,
        )

    def dx(k, src_z, src_x):
        owner = src_z * nx + src_x
        return pltpu.make_async_remote_copy(
            src_ref=dall.at[owner],
            dst_ref=dall.at[owner],
            send_sem=dx_send.at[k - 1],
            recv_sem=dx_recv.at[nx - k - 1],
            device_id=(z * nx + xpeer(k), t),
            device_id_type=MESH,
        )

    for k in range(1, nz):
        dz(k, z).start()
    for m in range(1, nx):
        dx(m, z, x).start()
    relays(1, *FIRST_C)
    turns(0, HOLD_X)
    relays(2, *SECOND_A)
    for k in range(1, nz):
        dz(k, zpeer(k)).wait_recv()
        for m in range(1, nx):
            dx(m, zpeer(k), x).start()
    relays(2, *SECOND_B)
    turns(HOLD_X, pieces)
    relay_others(1, inner)
    relays(3, *THIRD_A)
    for step in range(2, nz):
        relay_others(step, inner)
    for m in range(1, nx):
        await_got(dx_recv.at[m - 1], dall.at[pl.ds(0, nz)])
    for j in range(nfs):
        dcat[pl.ds(j * share, share), :] = dall[j].astype(f32)
    direction = dcat[...].astype(bf16)

    turned = jnp.dot(gram_high[...], direction, preferred_element_type=f32)
    turned += jnp.dot(gram_low[...], direction, preferred_element_type=f32)
    squares = jnp.sum((turned * dcat[...]).reshape(rank // 8, 8, cols), axis=0)
    squares = jnp.sum(squares, axis=0, keepdims=True)
    squares = jnp.maximum(squares, 0.0)
    gate_sum = jnp.sum(squares[:, :cg], axis=1, keepdims=True)
    value_sum = jnp.sum(squares[:, cg:], axis=1, keepdims=True)
    sums[t, 0] = jnp.broadcast_to(gate_sum, (8, 128))
    sums[t, 1] = jnp.broadcast_to(value_sum, (8, 128))

    def tp(k, src_t):
        return pltpu.make_async_remote_copy(
            src_ref=sums.at[src_t],
            dst_ref=sums.at[src_t],
            send_sem=t_send.at[0],
            recv_sem=t_recv.at[0],
            device_id=(f, lax.rem(t + k, nt)),
            device_id_type=MESH,
        )

    for k in range(1, nt):
        tp(k, t).start()
    def expand(j, carry):
        at = pl.ds(pl.multiple_of(j * rows, rows), rows)
        updates[at, :] = jnp.dot(pv[at, :], direction, preferred_element_type=f32)
        return carry

    lax.fori_loop(0, nfs // 2, expand, 0, unroll=2)
    relays(3, *THIRD_B)
    lax.fori_loop(nfs // 2, nfs, expand, 0, unroll=2)
    relays(3, *THIRD_C)
    for step in range(4, nz):
        relays(step, 0, pieces, 0, pieces)
    for way in (1, -1):

        @pl.when(jnp.logical_and(valid(z - way), at_end(z - way)))
        def _():
            for p in range(cross_end, cross_most):
                for k in range(1, nx):
                    wz(way, z - way, k, p, z - way, True).wait_recv()
            await_got(wz_recv.at[lax.rem(nz - way, nz) - 1, pieces], wall.at[pl.ds(0, (nx - 1) * (pieces - cross_most))])
    await_got(t_recv.at[0], sums.at[pl.ds(0, nt - 1)])
    whole = sums[0]
    for k in range(1, nt):
        whole = whole + sums[k]
    entries = nfs * rows * nt
    gscale = (1.0 / (jnp.sqrt(whole[0] / (entries * cg)) + rms_floor))[0:1, 0:1]
    vscale = (1.0 / (jnp.sqrt(whole[1] / (entries * cv)) + rms_floor))[0:1, 0:1]

    at = pl.ds(pl.multiple_of(f * rows, rows), rows)
    gstep = updates[at, :cg] * gscale
    vstep = updates[at, cg:] * vscale
    gsteps[...] = gstep
    vsteps[...] = vstep
    new_gw[...] = gw[...] - learn_rate * gstep
    new_vw[...] = vw[...] - learn_rate * vstep

    def finish(j, p):
        at = pl.ds(pl.multiple_of(j * rows + p * part, part), part)
        held = wall[j * pieces + p].astype(f32)
        update = updates[at, :]
        gcopy[at, :] = (held[:, :cg] - learn_rate * (update[:, :cg] * gscale)).astype(bf16)
        vcopy[at, :] = (held[:, cg:] - learn_rate * (update[:, cg:] * vscale)).astype(bf16)

    def finish_block(j, lo, hi):
        def body(p, carry):
            finish(j, p)
            return carry

        lax.fori_loop(lo, hi, body, 0, unroll=True)

    for zi in range(nz):
        finish_block(zi * nx + x, 0, pieces)
    for k in range(1, nx):
        finish_block(z * nx + xpeer(k), 0, pieces)

    @pl.when(inner)
    def _():
        await_got(rz_send.at[0], zsrc.at[pl.ds(0, nz - 1)])
        for m in range(1, nx):
            await_got(rx_send.at[m - 1], rsrc.at[0])

    @pl.when(end)
    def _():
        await_got(hand_send.at[0], handed.at[pl.ds(0, nz - 1)])
        for m in range(1, nx):
            await_got(rx_send.at[m - 1], rsrc.at[0, 0])

    await_got(dz_send.at[0], dall.at[pl.ds(0, nz - 1)])
    for m in range(1, nx):
        await_got(dx_send.at[m - 1], dall.at[pl.ds(0, nz)])
    await_got(t_send.at[0], sums.at[pl.ds(0, nt - 1)])
    for step in range(max(nz - 1, 1)):
        sent(step)
    for step in range(1, nz):
        relay_others(step, end)
    if cross_least:
        for zi in range(1, nz):
            for k in range(1, nx):
                finish_block(zpeer(zi) * nx + xpeer(k), 0, cross_least)
    for step in range(1, nz):
        for p in range(cross_least, pieces):
            for way in (1, -1):
                src_z = z - way * step

                @pl.when(valid(src_z))
                def _():
                    for k in range(1, nx):
                        group = group_of(p)
                        whole_row = jnp.logical_not(at_end(src_z))
                        sem = wx_recv.at[k - 1, lax.rem(src_z - z + nz, nz) - 1, group]
                        if p == cross_least:
                            for case, first in ((at_end(src_z), cross_end), (whole_row, cross_inner)):
                                if step == 1 and case is not whole_row:
                                    continue

                                @pl.when(case)
                                def _():
                                    await_got(sem, wall.at[pl.ds(0, pieces - SINGLES - first)])

                        elif group:

                            @pl.when(jnp.logical_not(rides(step, p, src_z)))
                            def _():
                                await_got(sem, wall.at[p])

                        finish(src_z * nx + xpeer(k), p)
    if nz > 1:
        sent(nz - 1)


def put_kernel(*refs):
    count = (len(refs) - 1) // 2
    sem = refs[-1]
    copies = [pltpu.make_async_copy(refs[i], refs[count + i], sem.at[i]) for i in range(count)]
    for copy in copies:
        copy.start()
    for copy in copies:
        copy.wait()


def per_device(nz, nx, nt, xin, gcot, fcot, scot, lam, proj, gw, gm, gs, vw, vm, vs):
    nfs = nz * nx
    rows, cg = gw.shape
    cv = vw.shape[1]
    cols = cg + cv
    depth, rank = proj.shape
    share = rank // nfs
    pieces = min(PIECES, rows // PIECE_ROWS)
    part = rows // pieces
    dma = pltpu.SemaphoreType.DMA
    shape = jax.ShapeDtypeStruct
    vmem = lambda a: pltpu.VMEM(a.shape, a.dtype)
    results = [
        shape((rows, cg), f32),
        shape((rows, cg), f32),
        shape((depth, cg), bf16),
        shape(gm.shape, f32),
        shape(gs.shape, f32),
        shape((rows, cv), f32),
        shape((rows, cv), f32),
        shape((depth, cv), bf16),
        shape(vm.shape, f32),
        shape(vs.shape, f32),
    ]
    arrays = [xin, gcot, fcot, scot, lam, proj, gw, gm, gs, vw, vm, vs]
    alone = cv == VDIM
    arrays = [
        a if alone and a is lam else pltpu.with_memory_space_constraint(a, pltpu.HBM)
        for a in arrays
    ]
    anywhere = pl.BlockSpec(memory_space=pl.ANY)
    inside = pl.BlockSpec(memory_space=pltpu.VMEM)
    held = pl.pallas_call(
        functools.partial(kernel, nz, nx, nt),
        out_shape=[vmem(a) for a in results],
        in_specs=[
            pl.BlockSpec(memory_space=pltpu.SMEM) if alone and a is lam else anywhere
            for a in (xin, gcot, fcot, scot, lam, proj, gw, gm, gs, vw, vm, vs)
        ],
        out_specs=[inside] * 10,
        scratch_shapes=[
            pltpu.SMEM(lam.shape, lam.dtype),
            vmem(xin),
            vmem(gcot),
            vmem(fcot),
            vmem(scot),
            vmem(proj),
            vmem(gw),
            vmem(vw),
            vmem(gm),
            vmem(gs),
            vmem(vm),
            vmem(vs),
            pltpu.VMEM((nfs * pieces, part, cols), bf16),
            pltpu.VMEM((rank, depth), bf16),
            pltpu.VMEM((rank, rank), bf16),
            pltpu.VMEM((rank, rank), bf16),
            pltpu.VMEM((rank, cols), f32),
            pltpu.VMEM((depth, cols), f32),
            pltpu.VMEM((nx, nz, share, cols), bf16),
            pltpu.VMEM((nx - 1, nz, share, cols), bf16),
            pltpu.VMEM((nz, share, cols), bf16),
            pltpu.VMEM((nz - 2, share, cols), bf16),
            pltpu.VMEM((nz, nx, share, cols), bf16),
            pltpu.VMEM((share, cols), f32),
            pltpu.VMEM((nfs, share, cols), bf16),
            pltpu.VMEM((rank, cols), f32),
            pltpu.VMEM((nt, 2, 8, 128), f32),
            dma((4,)),
            dma((DEPTH,)),
            dma((2, nz)),
            dma((nz - 1, pieces + 1)),
            dma((nz - 1, (nx - 1) * max(pieces * max(CROSS_INNER, CROSS_END) // PIECES, 1))),
            dma((nx - 1, nz)),
            dma((nx - 1, nz - 1, SINGLES + 1)),
            dma((nx - 1, 2)),
            dma((nx - 1,)),
            dma((nx - 1, nz)),
            dma((1,)),
            dma((1,)),
            dma((1,)),
            dma((nz,)),
            dma((nx - 1,)),
            dma((nx - 1,)),
            dma((1,)),
            dma((1,)),
            pltpu.SemaphoreType.REGULAR((nz - 2,)),
            dma((1,)),
            dma((nz,)),
        ],
        compiler_params=pltpu.CompilerParams(
            collective_id=0, has_side_effects=True, vmem_limit_bytes=40 * 1024 * 1024
        ),
    )(*arrays)
    return tuple(
        pl.pallas_call(
            put_kernel,
            out_shape=results,
            in_specs=[inside] * 10,
            out_specs=[anywhere] * 10,
            scratch_shapes=[dma((10,))],
            compiler_params=pltpu.CompilerParams(vmem_limit_bytes=8 * 1024 * 1024),
        )(*held)
    )


def solution(mesh):
    nz, nx = factor_fs(mesh.shape["fs"])
    assert nz > 3 and nx > 1
    split, whole = P("fs", "tp"), P(None, "tp")
    placed = (P("fs", None), split, split, split, P("tp"), P()) + (split,) * 6
    return jax.shard_map(
        functools.partial(per_device, nz, nx, mesh.shape["tp"]),
        mesh=mesh,
        in_specs=placed,
        out_specs=(split, split, whole, split, split, split, split, whole, split, split),
        check_vma=False,
    )
```
